32 devices in a mesh: fs: 4 (over y, x), tp: 8 (over z, core).
Axes of the slice: x: 2, y: 2, z: 4, core: 2. Of those that a mesh axis runs over, the one named last changes fastest.
Arguments:
- prompt: bfloat16 [4096, 2048], P(('fs', 'tp')), may hold values from -6 to 6
- norm_gain: float32 [2048], P('tp'), may hold values from 0.1 to 1.9
- gate_master: float32 [8, 2, 512, 2048], P(None, None, 'fs', 'tp'), may hold values from -0.125 to 0.125
- up_master: float32 [8, 2, 512, 2048], P(None, None, 'fs', 'tp'), may hold values from -0.125 to 0.125
- down_master: float32 [8, 2, 512, 2048], P(None, None, 'fs', 'tp'), may hold values from -0.25 to 0.25
- group_pick: int32 [4096, 1], P(('fs', 'tp')), may hold values from 0 to 7; in each aligned block of 128 rows (0 to 127, 128 to 255, ...) at most 32 rows name the same one
- route_weight: bfloat16 [4096, 2], P(('fs', 'tp')), may hold values from 0.099609375 to 1
Outputs:
- gate_serve: bfloat16 [8, 2, 512, 2048], P('tp', None, 'fs')
- up_serve: bfloat16 [8, 2, 512, 2048], P('tp', None, 'fs')
- down_serve: bfloat16 [8, 2, 512, 2048], P('tp', None, 'fs')
- mixed: bfloat16 [4096, 2048], P(('fs', 'tp'))
The draws below stay inside these ranges and needn't reach their ends.
Inputs may be any that keep to these rules, and one draw needn't show every extreme that they name: `group_pick`: in the rows of one device no group is named by more than 32 rows, and in every draw some device's rows name one group exactly 32 times.
All inputs are finite; a program needn't handle non-finite values.
Results may differ from the reference program's by a relative error of at most 0.0081.
Values may be sent and summed in bfloat16 or wider, within the bound.
No kernel may reach another device: no remote copies, remote signals or barrier semaphores. Data moves between devices by JAX's collectives and lax.ppermute only.
A program may use at most 64 MiB of HBM per device.

```python
import math
import jax
import jax.numpy as jnp
import numpy as np
from jax import lax

D = 2048
HID = 512
EXP_GRP = 2
TOK_DEV = 128
GROUPS = 8
CAP = 32
TOKENS = 4096


def steps_of(key, shape, shards, smallest, high):
    gain = 1.0
    for position, shards_of in shards:
        heights = jax.random.uniform(jax.random.fold_in(jax.random.fold_in(key, 6), position), (shards_of,), jnp.float32, smallest / len(shards), high / len(shards))
        gain = gain * jnp.repeat(jnp.exp(heights), shape[position] // shards_of).reshape((-1,) + (1,) * (len(shape) - 1 - position))
    return gain


def assign_block(rng, own, number, rows, number_of, top, bound, skew):
    ranking = jax.random.permutation(rng, number_of)
    packed, ordinary = load_shares(number_of, rows * top, bound, skew, True), load_shares(number_of, rows * top, bound, skew, False)
    places = jnp.arange(number_of)

    def named(sizes, rotation):
        used = int((sizes > 0).sum())
        fixed = max(1, used // 4)
        passed = fixed + (places - fixed + rotation * (used - fixed)) % max(1, number_of - fixed)
        return jnp.zeros((number_of,), jnp.int32).at[ranking[jnp.where(places < fixed, places, passed)]].set(jnp.asarray(sizes, jnp.int32))

    sizes = jnp.where(number % 4 == 0, named(packed, number // 4), named(ordinary, number - number // 4 - 1))
    mixed = jax.random.permutation(jax.random.fold_in(own, 3), number_of)
    source_of, taker = mixed[0:number_of // 2 * 2:2], mixed[1:number_of // 2 * 2:2]
    slack = jnp.minimum(sizes[source_of] - 1, bound - sizes[taker]) // 2
    slack = jnp.where((source_of == ranking[0]) | (taker == ranking[0]) | (sizes[taker] == 0), 0, jnp.maximum(slack, 0))
    passed = jax.random.randint(jax.random.fold_in(own, 4), (number_of // 2,), 0, 1 << 20) % (slack + 1)
    sizes = sizes.at[source_of].add(-passed).at[taker].add(passed)
    items = jnp.searchsorted(jnp.cumsum(sizes), jnp.arange(rows * top), side="right").astype(jnp.int32)
    grid = items.reshape(top, rows).T
    grid = grid[jax.random.permutation(jax.random.fold_in(own, 1), rows)]
    rotation = jax.random.randint(jax.random.fold_in(own, 2), (rows, 1), 0, top)
    return jnp.take_along_axis(grid, (jnp.arange(top)[None, :] + rotation) % top, axis=1)


def load_shares(amount, total, reach, skew, full):
    loads = [(1 << 20) // math.isqrt(standing ** skew) + 1 for standing in range(1, amount + 1)]
    largest = reach if full else min(reach, max(-(-total // amount), total * loads[0] // sum(loads)))
    least = 1 if total - largest >= amount - 1 else 0
    given, surplus = [largest] + [least] * (amount - 1), total - largest - least * (amount - 1)
    while surplus > 0:
        movable = [i for i in range(1, amount) if given[i] < largest] or [i for i in range(1, amount) if given[i] < reach]
        whole, budget = sum([loads[i] for i in movable]), surplus
        for i in movable:
            addition = min(reach - given[i], max(1, budget * loads[i] // whole), surplus)
            given[i] = given[i] + addition
            surplus = surplus - addition
    return np.array(given)


def normal_values(own_key, dims, spread, limit, pieces=(), kind=jnp.bfloat16):
    entries = spread * jax.random.normal(own_key, dims, jnp.float32)
    if pieces:
        entries = entries * steps_of(own_key, dims, pieces, -0.22, 0.18)
    return jnp.clip(entries, -limit, limit).astype(kind)


def setup_inputs(seed: int = 0) -> dict:
    splits = jax.random.split(jax.random.key(seed), 8)
    prompt = normal_values(splits[0], (TOKENS, D), 1.0, 6.0, ((0, 32),))
    norm_gain = jnp.clip(1.0 + 0.18 * jax.random.normal(splits[1], (D,), jnp.float32), 0.1, 1.9)
    gate_master = normal_values(splits[2], (GROUPS, EXP_GRP, HID, D), D ** -0.5, 0.125, ((2, 4), (3, 8)), jnp.float32)
    up_master = normal_values(splits[3], (GROUPS, EXP_GRP, HID, D), D ** -0.5, 0.125, ((2, 4), (3, 8)), jnp.float32)
    down_master = normal_values(splits[4], (GROUPS, EXP_GRP, HID, D), HID ** -0.5, 0.25, ((2, 4), (3, 8)), jnp.float32)
    group_pick_keys = jax.random.split(jax.random.fold_in(splits[5], 1), TOKENS // TOK_DEV)
    group_pick_turns = jax.random.permutation(jax.random.fold_in(splits[5], 3), TOKENS // TOK_DEV)
    group_pick = jax.vmap(lambda own, number: assign_block(jax.random.fold_in(splits[5], 2), own, number, TOK_DEV, GROUPS, 1, CAP, 2))(group_pick_keys, group_pick_turns).reshape((TOKENS, 1))
    route_weight = jnp.clip(jnp.exp(math.log(1.0) - 2.306499 * jax.random.uniform(splits[6], (TOKENS, EXP_GRP), jnp.float32) ** steps_of(splits[6], (TOKENS, EXP_GRP), ((0, 32),), -0.2, 0.2)), 0.099609375, 1.0).astype(jnp.bfloat16)
    return dict(prompt=prompt, norm_gain=norm_gain, gate_master=gate_master, up_master=up_master, down_master=down_master, group_pick=group_pick, route_weight=route_weight)


EPS = 1e-06

def reference(prompt, norm_gain, gate_master, up_master, down_master, group_pick, route_weight):
    gate_serve = (gate_master * norm_gain).astype(jnp.bfloat16)
    up_serve = (up_master * norm_gain).astype(jnp.bfloat16)
    down_serve = down_master.astype(jnp.bfloat16)
    values = prompt.astype(jnp.float32)
    normed = (values * lax.rsqrt(lax.optimization_barrier(jnp.mean(values * values, axis=1, keepdims=True)) + EPS)).astype(jnp.bfloat16)
    chosen = group_pick[:, 0].astype(jnp.int32)
    order = jnp.argsort(chosen, stable=True).astype(jnp.int32)
    member = (chosen[:, None] == jnp.arange(GROUPS, dtype=jnp.int32)[None, :]).astype(jnp.int32)
    counts = lax.optimization_barrier(jnp.sum(member, axis=0)).astype(jnp.int32)
    starts = (jnp.cumsum(counts) - counts).astype(jnp.int32)
    row_bound = CAP * (TOKENS // TOK_DEV)
    slot_ids = jnp.arange(row_bound, dtype=jnp.int32)

    def one_group(running, group_index):
        slot_place = jnp.minimum(starts[group_index] + slot_ids, TOKENS - 1).astype(jnp.int32)
        token_ids = order[slot_place].astype(jnp.int32)
        is_valid = slot_ids < counts[group_index]
        group_rows = normed[token_ids].astype(jnp.float32)
        weights = jnp.where(is_valid[:, None], route_weight[token_ids].astype(jnp.float32), 0.0)
        gate_pre = jnp.einsum('sd,ehd->seh', group_rows, gate_serve[group_index].astype(jnp.float32))
        up_pre = jnp.einsum('sd,ehd->seh', group_rows, up_serve[group_index].astype(jnp.float32))
        hidden = (weights[:, :, None] * (jax.nn.silu(gate_pre) * up_pre)).astype(jnp.bfloat16)
        expert_out = jnp.einsum('seh,ehd->sd', hidden.astype(jnp.float32), down_serve[group_index].astype(jnp.float32)).astype(jnp.bfloat16)
        expert_out = jnp.where(is_valid[:, None], expert_out, jnp.zeros_like(expert_out))
        running = running.at[token_ids].add(expert_out)
        return (running, None)
    mixed, _ = lax.scan(one_group, jnp.zeros((TOKENS, D), jnp.bfloat16), jnp.arange(GROUPS, dtype=jnp.int32))
    return (gate_serve, up_serve, down_serve, mixed)
```

```python
import functools

import jax
import jax.numpy as jnp
from jax import lax
from jax.experimental import pallas as pl
from jax.experimental.pallas import tpu as pltpu
from jax.sharding import PartitionSpec as P

EPS = 1e-06
LANES = 128
VMEM = pl.BlockSpec(memory_space=pltpu.VMEM)


def nt_dot(left, right):
    return lax.dot_general(left, right, (((1,), (1,)), ((), ())), preferred_element_type=jnp.float32)


def cost(flops, moved):
    return pl.CostEstimate(flops=int(flops), bytes_accessed=int(moved), transcendentals=0)


def swap(value, axis, distance):
    count = lax.axis_size(axis)
    return lax.ppermute(value, axis, [(i, i ^ distance) for i in range(count)])


def route_kernel(cap, me_ref, prompt_ref, pick_ref, weight_ref, *out_refs):
    placing_ref, blocks = out_refs[0], out_refs[1:]
    slots, tokens = placing_ref.shape
    width = prompt_ref.shape[1]
    values = prompt_ref[...].astype(jnp.float32)
    scale = lax.rsqrt(jnp.mean(values * values, axis=1, keepdims=True) + EPS)
    normed = (values * scale).astype(jnp.bfloat16)
    distance = pick_ref[...] ^ me_ref[0]
    count = max(8, len(blocks))
    member = (lax.broadcasted_iota(jnp.int32, (count, tokens), 0) == distance).astype(jnp.float32)
    before = lax.broadcasted_iota(jnp.int32, (tokens, tokens), 0) < lax.broadcasted_iota(
        jnp.int32, (tokens, tokens), 1
    )
    earlier = jnp.dot(
        member.astype(jnp.bfloat16), before.astype(jnp.float32).astype(jnp.bfloat16),
        preferred_element_type=jnp.float32,
    )
    rank = jnp.sum(earlier * member, axis=0, keepdims=True).astype(jnp.int32)
    target = distance * cap + rank
    placing = (lax.broadcasted_iota(jnp.int32, (slots, tokens), 0) == target).astype(jnp.float32)
    placing = placing.astype(jnp.bfloat16)
    placing_ref[...] = placing
    weights = weight_ref[...].astype(jnp.float32)
    experts = weights.shape[0]
    row = lax.broadcasted_iota(jnp.int32, (LANES, tokens), 0)
    spread = jnp.zeros((LANES, tokens), jnp.float32)
    for x in range(experts):
        spread = jnp.where(row == x, weights[x : x + 1, :], spread)
    placed_weights = nt_dot(placing, spread.astype(jnp.bfloat16)).astype(jnp.bfloat16)
    rows = jnp.dot(placing, normed, preferred_element_type=jnp.float32).astype(jnp.bfloat16)
    for d, block in enumerate(blocks):
        block[:, :width] = rows[d * cap : (d + 1) * cap]
        block[:, width:] = placed_weights[d * cap : (d + 1) * cap]


def route(me, prompt, group_pick, route_weight):
    tokens, width = prompt.shape
    groups = lax.axis_size("tp")
    cap = 2 * tokens // groups
    block = jax.ShapeDtypeStruct((cap, width + LANES), jnp.bfloat16)
    outs = pl.pallas_call(
        functools.partial(route_kernel, cap),
        out_shape=[jax.ShapeDtypeStruct((groups * cap, tokens), jnp.bfloat16)] + [block] * groups,
        in_specs=[pl.BlockSpec(memory_space=pltpu.SMEM)] + [VMEM] * 3,
        out_specs=[VMEM] * (groups + 1),
        cost_estimate=cost(2 * groups * cap * tokens * width, 2 * tokens * width * 6),
        name="route",
    )(me, prompt, group_pick.reshape(1, tokens), route_weight.T)
    return outs[0], outs[1:]


def round_kernel(scaled, me_ref, gain_ref, *refs):
    masters, blocks = refs[: len(scaled)], refs[len(scaled) :]
    gain = gain_ref[...].reshape(1, 1, -1)
    for d, block in enumerate(blocks):
        for k, master in enumerate(masters):
            values = master[me_ref[0] ^ d]
            if scaled[k]:
                values = values * gain
            block[k] = values.astype(jnp.bfloat16)


def rounded(me, gain, masters, scaled):
    groups, experts, units, part = masters[0].shape
    block = jax.ShapeDtypeStruct((len(masters), experts, units, part), jnp.bfloat16)
    size = len(masters) * groups * experts * units * part
    return pl.pallas_call(
        functools.partial(round_kernel, scaled),
        out_shape=[block] * groups,
        in_specs=[pl.BlockSpec(memory_space=pltpu.SMEM)] + [VMEM] * (1 + len(masters)),
        out_specs=[VMEM] * groups,
        cost_estimate=cost(4 * size, 6 * size),
        name="rounding",
    )(me, gain.reshape(1, -1), *masters)


def joined(me, blocks, which):
    count = len(blocks)
    kinds, experts, units, part = blocks[0].shape
    if part % LANES:
        order = jnp.stack([block[which] for block in blocks])[me[0] ^ jnp.arange(count)]
        return jnp.moveaxis(order, 0, 2).reshape(1, experts, units, count * part)

    def kernel(me_ref, *refs):
        ins, out_ref, sems = refs[:count], refs[count], refs[count + 1]
        copies = []
        for d in range(count):
            start = pl.multiple_of((me_ref[0] ^ d) * part, part)
            copies.append(
                pltpu.make_async_copy(
                    ins[d].at[which], out_ref.at[0, :, :, pl.ds(start, part)], sems.at[d]
                )
            )
        for copy in copies:
            copy.start()
        for copy in copies:
            copy.wait()

    size = count * experts * units * part
    return pl.pallas_call(
        kernel,
        out_shape=jax.ShapeDtypeStruct((1, experts, units, count * part), jnp.bfloat16),
        in_specs=[pl.BlockSpec(memory_space=pltpu.SMEM)] + [VMEM] * count,
        out_specs=pl.BlockSpec(memory_space=pl.ANY),
        scratch_shapes=[pltpu.SemaphoreType.DMA((count,))],
        cost_estimate=cost(4 * size, 4 * size),
        name="joining",
    )(me, *blocks)


def gathered(first, second, axis):
    count = lax.axis_size(axis)
    firsts, seconds = [first], [second]
    for e in range(1, count):
        low, high = e & -e, 1 << (e.bit_length() - 1)
        firsts.append(swap(firsts[e ^ low], axis, low))
        seconds.append(swap(seconds[e ^ high], axis, high))
    return firsts, seconds


def pre_kernel(matrix_ref, *refs):
    count = len(refs) // 2
    matrix = matrix_ref[...]
    for rows_ref, out_ref in zip(refs[:count], refs[count:]):
        out_ref[...] = nt_dot(rows_ref[...], matrix)


def gate_pre(rows, matrix):
    units, width = matrix.shape
    count = rows[0].shape[0]
    return pl.pallas_call(
        pre_kernel,
        out_shape=[jax.ShapeDtypeStruct((count, units), jnp.float32)] * len(rows),
        in_specs=[VMEM] * (1 + len(rows)),
        out_specs=[VMEM] * len(rows),
        cost_estimate=cost(2 * len(rows) * count * units * width, 2 * len(rows) * count * width),
        name="gate",
    )(matrix, *rows)


def active_kernel(count, matrix_ref, *refs):
    rows, gates, outs = refs[:count], refs[count : 2 * count], refs[2 * count :]
    matrix = matrix_ref[...]
    half = rows[0].shape[0]
    for e in range(count // 2):
        for h in range(2):
            up = nt_dot(rows[2 * e + h][...], matrix)
            gate = gates[2 * e + h][...]
            silu = gate / (1.0 + jnp.exp(-gate))
            outs[e][h * half : (h + 1) * half, :] = (silu * up).astype(jnp.bfloat16)


def active_units(rows, gates, matrix):
    units, width = matrix.shape
    half = rows[0].shape[0]
    count = len(rows)
    return pl.pallas_call(
        functools.partial(active_kernel, count),
        out_shape=[jax.ShapeDtypeStruct((2 * half, units), jnp.bfloat16)] * (count // 2),
        in_specs=[VMEM] * (1 + 2 * count),
        out_specs=[VMEM] * (count // 2),
        cost_estimate=cost(2 * count * half * units * width, 2 * count * half * width),
        name="active",
    )(matrix, *rows, *gates)


def mix_kernel(members, experts, weight_ref, *refs):
    hiddens, downs = refs[:members], refs[members : members * (1 + experts)]
    outs = refs[members * (1 + experts) :]
    cap = outs[0].shape[0]
    units = downs[0].shape[0]
    total = None
    for x in range(experts):
        hidden = jnp.concatenate([h[:, x * units : (x + 1) * units] for h in hiddens], axis=1)
        down = jnp.concatenate([d[...] for d in downs[x * members : (x + 1) * members]], axis=0)
        term = jnp.dot(hidden, down, preferred_element_type=jnp.float32)
        term = term * weight_ref[:, x : x + 1].astype(jnp.float32)
        total = term if total is None else total + term
    total = total.astype(jnp.bfloat16)
    for d, out in enumerate(outs):
        out[...] = total[d * cap : (d + 1) * cap]


def mixed_rows(weights, hiddens, downs, groups, chunk, chunks):
    members, experts = len(hiddens), len(downs)
    slots = weights.shape[0]
    units, width = downs[0][0].shape
    step = width // chunks
    cap = slots // groups
    down_spec = pl.BlockSpec((units, step), lambda i: (0, chunk))
    whole = lambda shape: pl.BlockSpec(shape, lambda i: (0,) * len(shape))
    return pl.pallas_call(
        functools.partial(mix_kernel, members, experts),
        grid=(1,),
        out_shape=[jax.ShapeDtypeStruct((cap, step), jnp.bfloat16)] * groups,
        in_specs=[whole(weights.shape)]
        + [whole(h.shape) for h in hiddens]
        + [down_spec] * (members * experts),
        out_specs=[whole((cap, step))] * groups,
        cost_estimate=cost(2 * slots * members * experts * units * step, 2 * members * experts * units * step),
        name="mixing",
    )(weights, *hiddens, *[d for group in downs for d in group])


def finish_kernel(chunks, placing_ref, *refs):
    out_ref, rows_ref = refs[-2], refs[-1]
    blocks = refs[:-2]
    per = len(blocks) // chunks
    cap, step = blocks[0].shape
    for k in range(chunks):
        for d in range(per):
            rows_ref[d * cap : (d + 1) * cap, k * step : (k + 1) * step] = blocks[k * per + d][...]
    out_ref[...] = lax.dot_general(
        placing_ref[...], rows_ref[...], (((0,), (0,)), ((), ())), preferred_element_type=jnp.float32
    ).astype(jnp.bfloat16)


def finished(placing, blocks, width):
    slots, tokens = placing.shape
    flat = [b for chunk in blocks for b in chunk]
    return pl.pallas_call(
        functools.partial(finish_kernel, len(blocks)),
        out_shape=jax.ShapeDtypeStruct((tokens, width), jnp.bfloat16),
        in_specs=[VMEM] * (1 + len(flat)),
        out_specs=VMEM,
        scratch_shapes=[pltpu.VMEM((slots, width), jnp.bfloat16)],
        cost_estimate=cost(2 * slots * tokens * width, 2 * slots * width),
        name="finish",
    )(placing, *flat)


def exchanged(blocks):
    far_first = sorted(range(1, len(blocks)), reverse=True)
    got = {d: swap(blocks[d], "tp", d) for d in far_first}
    return [blocks[0]] + [got[d] for d in range(1, len(blocks))]


def per_device(prompt, norm_gain, gate_master, up_master, down_master, group_pick, route_weight):
    groups, members = lax.axis_size("tp"), lax.axis_size("fs")
    width = prompt.shape[1]
    experts, units = gate_master.shape[1], gate_master.shape[2]
    chunks = 2
    me = lax.axis_index("tp").astype(jnp.int32).reshape(1)
    placing, send = route(me, prompt, group_pick, route_weight)
    rows = exchanged(send)
    gate_down = exchanged(rounded(me, norm_gain, [gate_master, down_master], [True, False]))
    up_only = exchanged(rounded(me, norm_gain, [up_master], [True]))

    half = groups // 2
    weights = jnp.concatenate([r[:, width:] for r in rows], axis=0)
    first = jnp.concatenate([r[:, :width] for r in rows[:half]], axis=0)
    second = jnp.concatenate([r[:, :width] for r in rows[half:]], axis=0)
    firsts, seconds = gathered(first, second, "fs")
    all_rows = [r for pair in zip(firsts, seconds) for r in pair]

    gate_serve = joined(me, gate_down, 0)
    down_serve = joined(me, gate_down, 1)
    downs = gathered(down_serve[0, 0], down_serve[0, 1], "fs")
    gates = gate_pre(all_rows, gate_serve.reshape(experts * units, width))
    up_serve = joined(me, up_only, 0)
    active = active_units(all_rows, gates, up_serve.reshape(experts * units, width))
    hiddens = [active[0]] + [swap(active[e], "fs", e) for e in range(1, members)]
    returned = [
        exchanged(mixed_rows(weights, hiddens, downs, groups, k, chunks)) for k in range(chunks)
    ]
    mixed = finished(placing, returned, width)
    return (gate_serve, up_serve, down_serve, mixed)


def solution(mesh):
    placed = (
        P(("fs", "tp"), None),
        P("tp"),
        P(None, None, "fs", "tp"),
        P(None, None, "fs", "tp"),
        P(None, None, "fs", "tp"),
        P(("fs", "tp"), None),
        P(("fs", "tp"), None),
    )
    return jax.shard_map(
        per_device,
        mesh=mesh,
        in_specs=placed,
        out_specs=(
            P("tp", None, "fs", None),
            P("tp", None, "fs", None),
            P("tp", None, "fs", None),
            P(("fs", "tp"), None),
        ),
        check_vma=False,
    )
```

```python
import functools

import jax
import jax.numpy as jnp
from jax import lax
from jax.experimental import pallas as pl
from jax.experimental.pallas import tpu as pltpu
from jax.sharding import PartitionSpec as P


EPS = 1e-06
LANES = 128
VMEM = pl.BlockSpec(memory_space=pltpu.VMEM)


def nt_dot(left, right):
    return lax.dot_general(left, right, (((1,), (1,)), ((), ())), preferred_element_type=jnp.float32)


def cost(flops, moved):
    return pl.CostEstimate(flops=int(flops), bytes_accessed=int(moved), transcendentals=0)


def swap(value, axis, distance):
    count = lax.axis_size(axis)
    return lax.ppermute(value, axis, [(i, i ^ distance) for i in range(count)])


def far_first(count):
    half = count // 2
    return list(range(half, count)) + list(range(2, half)) + ([1] if half > 1 else [])


def route_kernel(cap, me_ref, prompt_ref, pick_ref, weight_ref, *out_refs):
    placing_ref, blocks = out_refs[0], out_refs[1:]
    slots, tokens = placing_ref.shape
    width = prompt_ref.shape[1]
    values = prompt_ref[...].astype(jnp.float32)
    scale = lax.rsqrt(jnp.mean(values * values, axis=1, keepdims=True) + EPS)
    normed = (values * scale).astype(jnp.bfloat16)
    distance = pick_ref[...] ^ me_ref[0]
    count = max(8, len(blocks))
    member = (lax.broadcasted_iota(jnp.int32, (count, tokens), 0) == distance).astype(jnp.float32)
    before = lax.broadcasted_iota(jnp.int32, (tokens, tokens), 0) < lax.broadcasted_iota(
        jnp.int32, (tokens, tokens), 1
    )
    earlier = jnp.dot(
        member.astype(jnp.bfloat16), before.astype(jnp.float32).astype(jnp.bfloat16),
        preferred_element_type=jnp.float32,
    )
    rank = jnp.sum(earlier * member, axis=0, keepdims=True).astype(jnp.int32)
    target = distance * cap + rank
    placing = (lax.broadcasted_iota(jnp.int32, (slots, tokens), 0) == target).astype(jnp.float32)
    placing = placing.astype(jnp.bfloat16)
    placing_ref[...] = placing
    weights = weight_ref[...].astype(jnp.float32)
    experts = weights.shape[0]
    row = lax.broadcasted_iota(jnp.int32, (LANES, tokens), 0)
    spread = jnp.zeros((LANES, tokens), jnp.float32)
    for x in range(experts):
        spread = jnp.where(row == x, weights[x : x + 1, :], spread)
    placed_weights = nt_dot(placing, spread.astype(jnp.bfloat16)).astype(jnp.bfloat16)
    rows = jnp.dot(placing, normed, preferred_element_type=jnp.float32).astype(jnp.bfloat16)
    for d, block in enumerate(blocks):
        block[:, :width] = rows[d * cap : (d + 1) * cap]
        block[:, width:] = placed_weights[d * cap : (d + 1) * cap]


def route(me, prompt, group_pick, route_weight):
    tokens, width = prompt.shape
    groups = lax.axis_size("tp")
    cap = 2 * tokens // groups
    block = jax.ShapeDtypeStruct((cap, width + LANES), jnp.bfloat16)
    outs = pl.pallas_call(
        functools.partial(route_kernel, cap),
        out_shape=[jax.ShapeDtypeStruct((groups * cap, tokens), jnp.bfloat16)] + [block] * groups,
        in_specs=[pl.BlockSpec(memory_space=pltpu.SMEM)] + [VMEM] * 3,
        out_specs=[VMEM] * (groups + 1),
        cost_estimate=cost(2 * groups * cap * tokens * width, 2 * tokens * width * 6),
        name="route",
    )(me, prompt, group_pick.reshape(1, tokens), route_weight.T)
    return outs[0], outs[1:]


def round_kernel(scaled, me_ref, gain_ref, master_ref, after_ref, *blocks):
    gain = gain_ref[...].reshape(1, 1, -1)
    for d, block in enumerate(blocks):
        values = master_ref[me_ref[0] ^ d]
        if scaled:
            values = values * gain
        block[...] = values.astype(jnp.bfloat16)


def rounded(me, gain, master, scaled, after):
    groups, experts, units, part = master.shape
    block = jax.ShapeDtypeStruct((experts, units, part), jnp.bfloat16)
    size = groups * experts * units * part
    return pl.pallas_call(
        functools.partial(round_kernel, scaled),
        out_shape=[block] * groups,
        in_specs=[pl.BlockSpec(memory_space=pltpu.SMEM)]
        + [VMEM] * 2
        + [pl.BlockSpec(memory_space=pl.ANY)],
        out_specs=[VMEM] * groups,
        cost_estimate=cost(4 * size, 6 * size),
        name="rounding",
    )(me, gain.reshape(1, -1), master, after)


def joined(me, blocks):
    count = len(blocks)
    experts, units, part = blocks[0].shape
    if part % LANES:
        order = jnp.stack(blocks)[me[0] ^ jnp.arange(count)]
        return jnp.moveaxis(order, 0, 2).reshape(1, experts, units, count * part)

    def kernel(me_ref, *refs):
        ins, out_ref, sems = refs[:count], refs[count], refs[count + 1]
        copies = []
        for d in range(count):
            start = pl.multiple_of((me_ref[0] ^ d) * part, part)
            copies.append(
                pltpu.make_async_copy(ins[d], out_ref.at[0, :, :, pl.ds(start, part)], sems.at[d])
            )
        for copy in copies:
            copy.start()
        for copy in copies:
            copy.wait()

    size = count * experts * units * part
    return pl.pallas_call(
        kernel,
        out_shape=jax.ShapeDtypeStruct((1, experts, units, count * part), jnp.bfloat16),
        in_specs=[pl.BlockSpec(memory_space=pltpu.SMEM)] + [VMEM] * count,
        out_specs=pl.BlockSpec(memory_space=pl.ANY),
        scratch_shapes=[pltpu.SemaphoreType.DMA((count,))],
        cost_estimate=cost(4 * size, 4 * size),
        name="joining",
    )(me, *blocks)


def stack_rows_kernel(width, *refs):
    blocks, rows_ref, weights_ref = refs[:-2], refs[-2], refs[-1]
    cap = blocks[0].shape[0]
    for d, block in enumerate(blocks):
        rows_ref[d * cap : (d + 1) * cap] = block[:, :width]
        weights_ref[d * cap : (d + 1) * cap] = block[:, width:]


def stacked_rows(blocks, width):
    count, cap = len(blocks), blocks[0].shape[0]
    return pl.pallas_call(
        functools.partial(stack_rows_kernel, width),
        out_shape=[
            jax.ShapeDtypeStruct((count * cap, width), jnp.bfloat16),
            jax.ShapeDtypeStruct((count * cap, LANES), jnp.bfloat16),
        ],
        in_specs=[VMEM] * count,
        out_specs=[VMEM] * 2,
        cost_estimate=cost(count * cap * width, 4 * count * cap * width),
        name="stack_rows",
    )(*blocks)


def stack_columns_kernel(*refs):
    experts = refs[0].shape[0]
    blocks, outs = refs[:-experts], refs[-experts:]
    part = blocks[0].shape[-1]
    for d, block in enumerate(blocks):
        for x, out in enumerate(outs):
            out[:, d * part : (d + 1) * part] = block[x]


def stacked_columns(blocks):
    count = len(blocks)
    experts, units, part = blocks[0].shape
    size = count * experts * units * part
    return pl.pallas_call(
        stack_columns_kernel,
        out_shape=[jax.ShapeDtypeStruct((units, count * part), jnp.bfloat16)] * experts,
        in_specs=[VMEM] * count,
        out_specs=[VMEM] * experts,
        cost_estimate=cost(size, 4 * size),
        name="stack_columns",
    )(*blocks)


def gathered(first, second, axis):
    count = lax.axis_size(axis)
    firsts, seconds = [first], [second]
    for e in range(1, count):
        low, high = e & -e, 1 << (e.bit_length() - 1)
        firsts.append(swap(firsts[e ^ low], axis, low))
        seconds.append(swap(seconds[e ^ high], axis, high))
    return firsts, seconds


def pre_kernel(matrix_ref, *refs):
    count = len(refs) // 2
    matrix = matrix_ref[...]
    for rows_ref, out_ref in zip(refs[:count], refs[count:]):
        out_ref[...] = nt_dot(rows_ref[...], matrix)


def gate_pre(rows, matrix):
    units, width = matrix.shape
    count = rows[0].shape[0]
    return pl.pallas_call(
        pre_kernel,
        out_shape=[jax.ShapeDtypeStruct((count, units), jnp.float32)] * len(rows),
        in_specs=[VMEM] * (1 + len(rows)),
        out_specs=[VMEM] * len(rows),
        cost_estimate=cost(2 * len(rows) * count * units * width, 2 * len(rows) * count * width),
        name="gate",
    )(matrix, *rows)


def active_kernel(count, parts, me_ref, *refs):
    pieces, refs = refs[:parts], refs[parts:]
    rows, gates, outs = refs[:count], refs[count : 2 * count], refs[2 * count : -1]
    matrix_ref = refs[-1]
    experts, units, part = pieces[0].shape
    for d, piece in enumerate(pieces):
        start = pl.multiple_of((me_ref[0] ^ d) * part, part)
        for x in range(experts):
            matrix_ref[x * units : (x + 1) * units, pl.ds(start, part)] = piece[x]
    matrix = matrix_ref[...]
    half = rows[0].shape[0]
    for e in range(count // 2):
        for h in range(2):
            up = nt_dot(rows[2 * e + h][...], matrix)
            gate = gates[2 * e + h][...]
            silu = gate / (1.0 + jnp.exp(-gate))
            outs[e][h * half : (h + 1) * half, :] = (silu * up).astype(jnp.bfloat16)


def active_units(me, rows, gates, pieces):
    if pieces[0].shape[-1] % LANES:
        pieces, me = [joined(me, pieces)[0]], jnp.zeros_like(me)
    experts, units, part = pieces[0].shape
    units, width = experts * units, part * len(pieces)
    half = rows[0].shape[0]
    count = len(rows)
    return pl.pallas_call(
        functools.partial(active_kernel, count, len(pieces)),
        out_shape=[jax.ShapeDtypeStruct((2 * half, units), jnp.bfloat16)] * (count // 2),
        in_specs=[pl.BlockSpec(memory_space=pltpu.SMEM)] + [VMEM] * (len(pieces) + 2 * count),
        out_specs=[VMEM] * (count // 2),
        scratch_shapes=[pltpu.VMEM((units, width), jnp.bfloat16)],
        cost_estimate=cost(2 * count * half * units * width, 2 * count * half * width),
        name="active",
    )(me, *pieces, *rows, *gates)


def mix_kernel(members, experts, near_ref, far_ref, *refs):
    hiddens, downs = refs[:members], refs[members : members * (1 + experts)]
    outs = refs[members * (1 + experts) :]
    cap = outs[0].shape[0]
    units = downs[0].shape[0]
    total = None
    for x in range(experts):
        hidden = jnp.concatenate([h[:, x * units : (x + 1) * units] for h in hiddens], axis=1)
        down = jnp.concatenate([d[...] for d in downs[x * members : (x + 1) * members]], axis=0)
        term = jnp.dot(hidden, down, preferred_element_type=jnp.float32)
        weight = jnp.concatenate([near_ref[:, x : x + 1], far_ref[:, x : x + 1]], axis=0)
        term = term * weight.astype(jnp.float32)
        total = term if total is None else total + term
    total = total.astype(jnp.bfloat16)
    for d, out in enumerate(outs):
        out[...] = total[d * cap : (d + 1) * cap]


def mixed_rows(weights, hiddens, downs, groups):
    members, experts = len(hiddens), len(downs)
    slots = hiddens[0].shape[0]
    units, width = downs[0][0].shape
    cap = slots // groups
    return pl.pallas_call(
        functools.partial(mix_kernel, members, experts),
        out_shape=[jax.ShapeDtypeStruct((cap, width), jnp.bfloat16)] * groups,
        in_specs=[VMEM] * (2 + members + members * experts),
        out_specs=[VMEM] * groups,
        cost_estimate=cost(
            2 * slots * members * experts * units * width, 2 * members * experts * units * width
        ),
        name="mixing",
    )(*weights, *hiddens, *[d for group in downs for d in group])


def finish_kernel(chunks, part, me_ref, placing_ref, *refs):
    out_ref, rows_ref = refs[-2], refs[-1]
    blocks = refs[:-2]
    per = len(blocks) // chunks
    cap, step = blocks[0].shape
    for c in range(chunks):
        for d in range(per):
            for k in range(step // part):
                start = pl.multiple_of((me_ref[0] ^ d ^ (c * (step // part) + k)) * part, part)
                rows_ref[d * cap : (d + 1) * cap, pl.ds(start, part)] = blocks[c * per + d][
                    :, k * part : (k + 1) * part
                ]
    out_ref[...] = lax.dot_general(
        placing_ref[...], rows_ref[...], (((0,), (0,)), ((), ())), preferred_element_type=jnp.float32
    ).astype(jnp.bfloat16)


def ordered(me, d, chunks, part):
    rows = jnp.concatenate(chunks, axis=1)
    cap, width = rows.shape
    count = width // part
    order = me[0] ^ d ^ jnp.arange(count)
    return rows.reshape(cap, count, part)[:, order].reshape(cap, width)


def finished(me, placing, chunks, part):
    slots, tokens = placing.shape
    width = sum(chunk[0].shape[1] for chunk in chunks)
    if part % LANES:
        rows = [ordered(me, d, [chunk[d] for chunk in chunks], part) for d in range(len(chunks[0]))]
        return lax.dot_general(
            placing, jnp.concatenate(rows), (((0,), (0,)), ((), ())), preferred_element_type=jnp.float32
        ).astype(jnp.bfloat16)
    flat = [b for chunk in chunks for b in chunk]
    return pl.pallas_call(
        functools.partial(finish_kernel, len(chunks), part),
        out_shape=jax.ShapeDtypeStruct((tokens, width), jnp.bfloat16),
        in_specs=[pl.BlockSpec(memory_space=pltpu.SMEM)] + [VMEM] * (1 + len(flat)),
        out_specs=VMEM,
        scratch_shapes=[pltpu.VMEM((slots, width), jnp.bfloat16)],
        cost_estimate=cost(2 * slots * tokens * width, 2 * slots * width),
        name="finish",
    )(me, placing, *flat)


def exchanged(blocks):
    got = {d: swap(blocks[d], "tp", d) for d in far_first(len(blocks))}
    return [blocks[0]] + [got[d] for d in range(1, len(blocks))]


def served(prompt, norm_gain, gate_master, up_master, down_master, group_pick, route_weight):
    groups, members = lax.axis_size("tp"), lax.axis_size("fs")
    width = prompt.shape[1]
    experts, units, part = gate_master.shape[1:]
    half = groups // 2
    me = lax.axis_index("tp").astype(jnp.int32).reshape(1)

    placing, send = route(me, prompt, group_pick, route_weight)
    rows = exchanged(send)
    gate_send = rounded(me, norm_gain, gate_master, True, placing)
    gate_parts = exchanged(gate_send)
    up_send = rounded(me, norm_gain, up_master, True, gate_send[0])
    up_parts = exchanged(up_send)
    down_send = rounded(me, norm_gain, down_master, False, up_send[0])
    down_parts = exchanged(down_send)

    near, near_weights = stacked_rows(rows[:half], width)
    far, far_weights = stacked_rows(rows[half:], width)
    weights = (near_weights, far_weights)
    firsts, seconds = gathered(near, far, "fs")
    all_rows = [r for pair in zip(firsts, seconds) for r in pair]
    near_down = gathered(*stacked_columns(down_parts[:half]), "fs")
    far_down = gathered(*stacked_columns(down_parts[half:]), "fs")

    gate_serve = joined(me, gate_parts)
    gates = gate_pre(all_rows, gate_serve.reshape(experts * units, width))
    active = active_units(me, all_rows, gates, up_parts)
    hiddens = [active[0]] + [swap(active[e], "fs", e) for e in range(1, members)]
    near_mix = mixed_rows(weights, hiddens, near_down, groups)
    near_back = exchanged(near_mix)
    far_mix = mixed_rows(weights, hiddens, far_down, groups)
    far_back = exchanged(far_mix)
    mixed = finished(me, placing, [near_back, far_back], part)
    up_serve = joined(me, up_parts)
    down_serve = joined(me, down_parts)
    return (gate_serve, up_serve, down_serve, mixed)


def solution(mesh):
    placed = (
        P(("fs", "tp"), None),
        P("tp"),
        P(None, None, "fs", "tp"),
        P(None, None, "fs", "tp"),
        P(None, None, "fs", "tp"),
        P(("fs", "tp"), None),
        P(("fs", "tp"), None),
    )
    return jax.shard_map(
        served,
        mesh=mesh,
        in_specs=placed,
        out_specs=(
            P("tp", None, "fs", None),
            P("tp", None, "fs", None),
            P("tp", None, "fs", None),
            P(("fs", "tp"), None),
        ),
        check_vma=False,
    )
```

```python
import functools

import jax
import jax.numpy as jnp
from jax import lax
from jax.experimental import pallas as pl
from jax.experimental.pallas import tpu as pltpu
from jax.sharding import PartitionSpec as P


EPS = 1e-06
LANES = 128
BLOCKS = 2
VMEM = pl.BlockSpec(memory_space=pltpu.VMEM)


def nt_dot(left, right):
    return lax.dot_general(left, right, (((1,), (1,)), ((), ())), preferred_element_type=jnp.float32)


def cost(flops, moved):
    return pl.CostEstimate(flops=int(flops), bytes_accessed=int(moved), transcendentals=0)


def swap(value, axis, distance):
    count = lax.axis_size(axis)
    return lax.ppermute(value, axis, [(i, i ^ distance) for i in range(count)])


def route_kernel(cap, me_ref, prompt_ref, pick_ref, weight_ref, *out_refs):
    placing_ref, blocks = out_refs[0], out_refs[1:]
    slots, tokens = placing_ref.shape
    width = prompt_ref.shape[1]
    values = prompt_ref[...].astype(jnp.float32)
    scale = lax.rsqrt(jnp.mean(values * values, axis=1, keepdims=True) + EPS)
    normed = (values * scale).astype(jnp.bfloat16)
    distance = pick_ref[...] ^ me_ref[0]
    count = max(8, len(blocks))
    member = (lax.broadcasted_iota(jnp.int32, (count, tokens), 0) == distance).astype(jnp.float32)
    before = lax.broadcasted_iota(jnp.int32, (tokens, tokens), 0) < lax.broadcasted_iota(
        jnp.int32, (tokens, tokens), 1
    )
    earlier = jnp.dot(
        member.astype(jnp.bfloat16), before.astype(jnp.float32).astype(jnp.bfloat16),
        preferred_element_type=jnp.float32,
    )
    rank = jnp.sum(earlier * member, axis=0, keepdims=True).astype(jnp.int32)
    target = distance * cap + rank
    placing = (lax.broadcasted_iota(jnp.int32, (slots, tokens), 0) == target).astype(jnp.float32)
    placing = placing.astype(jnp.bfloat16)
    placing_ref[...] = placing
    weights = weight_ref[...].astype(jnp.float32)
    experts = weights.shape[0]
    row = lax.broadcasted_iota(jnp.int32, (LANES, tokens), 0)
    spread = jnp.zeros((LANES, tokens), jnp.float32)
    for x in range(experts):
        spread = jnp.where(row == x, weights[x : x + 1, :], spread)
    placed_weights = nt_dot(placing, spread.astype(jnp.bfloat16)).astype(jnp.bfloat16)
    rows = jnp.dot(placing, normed, preferred_element_type=jnp.float32).astype(jnp.bfloat16)
    for d, block in enumerate(blocks):
        block[:, :width] = rows[d * cap : (d + 1) * cap]
        block[:, width:] = placed_weights[d * cap : (d + 1) * cap]


def route(me, prompt, group_pick, route_weight):
    tokens, width = prompt.shape
    groups = lax.axis_size("tp")
    cap = 2 * tokens // groups
    block = jax.ShapeDtypeStruct((cap, width + LANES), jnp.bfloat16)
    outs = pl.pallas_call(
        functools.partial(route_kernel, cap),
        out_shape=[jax.ShapeDtypeStruct((groups * cap, tokens), jnp.bfloat16)] + [block] * groups,
        in_specs=[pl.BlockSpec(memory_space=pltpu.SMEM)] + [VMEM] * 3,
        out_specs=[VMEM] * (groups + 1),
        cost_estimate=cost(2 * groups * cap * tokens * width, 2 * tokens * width * 6),
        name="route",
    )(me, prompt, group_pick.reshape(1, tokens), route_weight.T)
    return outs[0], outs[1:]


def round_kernel(half, me_ref, gain_ref, gate_ref, up_ref, down_ref, *blocks):
    gain = gain_ref[...].reshape(1, 1, -1)
    near, far = blocks[:half], blocks[half:]
    for d in range(half + len(far) // 2):
        group = me_ref[0] ^ d
        pair, down = (near[d], near[d].at[2]) if d < half else (far[2 * (d - half)], far[2 * (d - half) + 1])
        pair[0] = (gate_ref[group] * gain).astype(jnp.bfloat16)
        pair[1] = (up_ref[group] * gain).astype(jnp.bfloat16)
        down[...] = down_ref[group].astype(jnp.bfloat16)


def rounded(me, gain, gate, up, down, after):
    groups, experts, units, part = gate.shape
    half = groups // 2
    shape = lambda *lead: jax.ShapeDtypeStruct((*lead, experts, units, part), jnp.bfloat16)
    size = 3 * groups * experts * units * part

    def kernel(me_ref, after_ref, *refs):
        round_kernel(half, me_ref, *refs)

    outs = pl.pallas_call(
        kernel,
        out_shape=[shape(3)] * half + [shape(2), shape()] * (groups - half),
        in_specs=[pl.BlockSpec(memory_space=pltpu.SMEM), pl.BlockSpec(memory_space=pl.ANY)] + [VMEM] * 4,
        out_specs=[VMEM] * (2 * groups - half),
        cost_estimate=cost(4 * size, 6 * size),
        name="rounding",
    )(me, after, gain.reshape(1, -1), gate, up, down)
    return outs[:half], outs[half::2], outs[half + 1 :: 2]


def parts_of(near, pairs, downs, which):
    if which == 2:
        return [ref[2] for ref in near] + list(downs)
    return [ref[which] for ref in near] + [ref[which] for ref in pairs]


def joined(me, near, pairs, downs):
    count = len(near) + len(pairs)
    _, experts, units, part = near[0].shape
    if part % LANES:
        order = me[0] ^ jnp.arange(count)
        outs = []
        for which in range(3):
            stack = jnp.stack(parts_of(near, pairs, downs, which))[order]
            outs.append(jnp.moveaxis(stack, 0, 2).reshape(1, experts, units, count * part))
        return outs
    sizes = (len(near), len(pairs), len(downs))

    def kernel(me_ref, *refs):
        ins, outs, sems = refs[: sum(sizes)], refs[sum(sizes) : -1], refs[-1]
        groups = ins[: sizes[0]], ins[sizes[0] : sizes[0] + sizes[1]], ins[sizes[0] + sizes[1] :]
        copies = []
        for which, out_ref in enumerate(outs):
            views = [[ref.at for ref in group] for group in groups[:2]]
            for d, piece in enumerate(parts_of(*views, groups[2], which)):
                start = pl.multiple_of((me_ref[0] ^ d) * part, part)
                copies.append(
                    pltpu.make_async_copy(
                        piece, out_ref.at[0, :, :, pl.ds(start, part)], sems.at[which, d]
                    )
                )
        for copy in copies:
            copy.start()
        for copy in copies:
            copy.wait()

    size = 3 * count * experts * units * part
    out = jax.ShapeDtypeStruct((1, experts, units, count * part), jnp.bfloat16)
    return pl.pallas_call(
        kernel,
        out_shape=[out] * 3,
        in_specs=[pl.BlockSpec(memory_space=pltpu.SMEM)] + [VMEM] * sum(sizes),
        out_specs=[pl.BlockSpec(memory_space=pl.ANY)] * 3,
        scratch_shapes=[pltpu.SemaphoreType.DMA((3, count))],
        cost_estimate=cost(4 * size, 4 * size),
        name="joining",
    )(me, *near, *pairs, *downs)


def stack_rows_kernel(width, *refs):
    blocks, rows_ref, weights_ref = refs[:-2], refs[-2], refs[-1]
    cap = blocks[0].shape[0]
    for d, block in enumerate(blocks):
        rows_ref[d * cap : (d + 1) * cap] = block[:, :width]
        weights_ref[d * cap : (d + 1) * cap] = block[:, width:]


def stacked_rows(blocks, width):
    count, cap = len(blocks), blocks[0].shape[0]
    return pl.pallas_call(
        functools.partial(stack_rows_kernel, width),
        out_shape=[
            jax.ShapeDtypeStruct((count * cap, width), jnp.bfloat16),
            jax.ShapeDtypeStruct((count * cap, LANES), jnp.bfloat16),
        ],
        in_specs=[VMEM] * count,
        out_specs=[VMEM] * 2,
        cost_estimate=cost(count * cap * width, 4 * count * cap * width),
        name="stack_rows",
    )(*blocks)


def stacked_columns(blocks, pieces):
    count = len(blocks)
    experts, units, part = blocks[0].shape[-3:]
    rows = experts * units // pieces

    def kernel(*refs):
        ins, outs = refs[:count], refs[count:]
        for d, block in enumerate(ins):
            piece = block.at[2] if len(block.shape) == 4 else block
            for x in range(experts):
                row = x * units % rows
                outs[x * units // rows][row : row + units, d * part : (d + 1) * part] = piece[x]

    size = count * experts * units * part
    return pl.pallas_call(
        kernel,
        out_shape=[jax.ShapeDtypeStruct((rows, count * part), jnp.bfloat16)] * pieces,
        in_specs=[VMEM] * count,
        out_specs=[VMEM] * pieces,
        cost_estimate=cost(size, 4 * size),
        name="stack_columns",
    )(*blocks)


def collected(value, axis):
    count = lax.axis_size(axis)
    return [value] + [swap(value, axis, e) for e in range(1, count)]


def gathered(first, second, axis):
    count = lax.axis_size(axis)
    firsts, seconds = [first], [second]
    for e in range(1, count):
        low, high = e & -e, 1 << (e.bit_length() - 1)
        firsts.append(swap(firsts[e ^ low], axis, low))
        seconds.append(swap(seconds[e ^ high], axis, high))
    return firsts, seconds


def active_kernel(first, parts, counts, me_ref, *refs):
    pieces, refs = refs[: counts[0]], refs[counts[0] :]
    rows, before, refs = refs[: counts[1]], refs[counts[1] : counts[1] + counts[2]], refs[sum(counts[1:3]) :]
    outs, (matrix_ref, rows_ref, sums_ref, sems) = refs[: counts[3]], refs[counts[3] :]
    _, experts, units, part = pieces[0].shape
    both = experts * units
    width = rows_ref.shape[2]
    place = lax.shift_right_logical(me_ref[0] ^ first, parts.bit_length() - 1)
    columns = pl.ds(pl.multiple_of(place * width, width), width)
    slots = rows[0].shape[0]
    spot = lambda b: rows_ref.at[b * slots // rows_ref.shape[1], pl.ds(b * slots % rows_ref.shape[1], slots)]
    copies = [
        pltpu.make_async_copy(ref.at[:, columns], spot(b), sems.at[0, b]) for b, ref in enumerate(rows)
    ]
    copies += [
        pltpu.make_async_copy(ref, sums_ref.at[b], sems.at[1, b]) for b, ref in enumerate(before)
    ]
    for copy in copies:
        copy.start()
    for d, piece in enumerate(pieces):
        start = pl.multiple_of(((me_ref[0] & (len(pieces) - 1)) ^ d) * part, part)
        for which in range(2):
            for x in range(experts):
                row = which * both + x * units
                matrix_ref[row : row + units, pl.ds(start, part)] = piece[which, x]
    group = rows_ref.shape[1] // slots
    for m in range(rows_ref.shape[0]):
        mine = range(m * group, (m + 1) * group)
        for b in mine:
            copies[b].wait()
        pre = nt_dot(rows_ref[m], matrix_ref[...])
        for b in mine:
            place = (b - m * group) * slots
            part_pre = pre[place : place + slots]
            if before:
                copies[len(rows) + b].wait()
                part_pre = part_pre + sums_ref[b]
            if len(outs) == len(rows):
                outs[b][...] = part_pre
            else:
                gate, up = part_pre[:, :both], part_pre[:, both:]
                silu = gate / (1.0 + jnp.exp(-gate))
                place = b % 2 * slots
                outs[b // 2][place : place + slots, :] = (silu * up).astype(jnp.bfloat16)


def active_units(me, rows, pieces, first, before, last):
    _, experts, units, part = pieces[0].shape
    parts = len(pieces)
    if part % LANES:
        order = (me[0] % parts) ^ jnp.arange(parts)
        stack = jnp.stack([block[:2] for block in pieces])[order]
        pieces = [jnp.moveaxis(stack, 0, 3).reshape(2, experts, units, parts * part)]
    slots, width = rows[0].shape[0], parts * part
    count, both = len(rows), experts * units
    if last:
        outs = [jax.ShapeDtypeStruct((2 * slots, both), jnp.bfloat16)] * (count // 2)
    else:
        outs = [jax.ShapeDtypeStruct((slots, 2 * both), jnp.float32)] * count
    counts = (len(pieces), count, len(before), len(outs))
    return pl.pallas_call(
        functools.partial(active_kernel, first, parts, counts),
        out_shape=outs,
        in_specs=[pl.BlockSpec(memory_space=pltpu.SMEM)]
        + [VMEM] * len(pieces)
        + [pl.BlockSpec(memory_space=pl.ANY)] * (count + len(before)),
        out_specs=[VMEM] * len(outs),
        scratch_shapes=[
            pltpu.VMEM((2 * both, width), jnp.bfloat16),
            pltpu.VMEM((BLOCKS, count * slots // BLOCKS, width), jnp.bfloat16),
            pltpu.VMEM((max(1, len(before)), slots, 2 * both), jnp.float32),
            pltpu.SemaphoreType.DMA((2, count)),
        ],
        cost_estimate=cost(4 * count * slots * both * width, 2 * count * slots * width),
        name="active",
    )(me, *pieces, *rows, *before)


def mix_kernel(members, experts, pieces, kept, near_ref, far_ref, *refs):
    hiddens, refs = refs[:members], refs[members:]
    number = members * sum(pieces)
    downs, kepts, outs = list(refs[:number]), refs[number : number + kept], refs[number + kept :]
    cap = outs[0].shape[0]
    for d, old in enumerate(kepts):
        outs[d][:, : old.shape[1]] = old[...]
    before = kepts[0].shape[1] if kept else 0
    begin = 0
    for piece in pieces:
        mine = [[downs.pop(0) for _ in range(piece)] for _ in range(members)]
        rows, width = mine[0][0].shape
        units = rows * piece // experts
        total = None
        for x in range(experts):
            row = x * units % rows
            hidden = jnp.concatenate([h[:, x * units : (x + 1) * units] for h in hiddens], axis=1)
            down = jnp.concatenate([d[x * units // rows][row : row + units] for d in mine], axis=0)
            term = jnp.dot(hidden, down, preferred_element_type=jnp.float32)
            weight = jnp.concatenate([near_ref[:, x : x + 1], far_ref[:, x : x + 1]], axis=0)
            term = term * weight.astype(jnp.float32)
            total = term if total is None else total + term
        total = total.astype(jnp.bfloat16)
        for d, out in enumerate(outs):
            place = begin + (before if d < kept else 0)
            out[:, place : place + width] = total[d * cap : (d + 1) * cap]
        begin += width


def mixed_rows(weights, hiddens, sets, kept, groups, experts):
    members = len(hiddens)
    slots = hiddens[0].shape[0]
    pieces = [len(downs[0]) for downs in sets]
    flat = [d for downs in sets for member in downs for d in member]
    width = sum(downs[0][0].shape[1] for downs in sets)
    cap = slots // groups
    before = kept[0].shape[1] if kept else 0
    out = lambda d: jax.ShapeDtypeStruct((cap, width + (before if d < len(kept) else 0)), jnp.bfloat16)
    size = members * hiddens[0].shape[1] * width
    return pl.pallas_call(
        functools.partial(mix_kernel, members, experts, pieces, len(kept)),
        out_shape=[out(d) for d in range(groups)],
        in_specs=[VMEM] * (2 + members + len(flat) + len(kept)),
        out_specs=[VMEM] * groups,
        cost_estimate=cost(2 * slots * size, 2 * size),
        name="mixing",
    )(*weights, *hiddens, *flat, *kept)


def finish_kernel(counts, part, me_ref, placing_ref, *refs):
    out_ref, rows_ref = refs[-2], refs[-1]
    blocks = list(refs[:-2])
    for d, count in enumerate(counts):
        base = 0
        for _ in range(count):
            block = blocks.pop(0)
            cap = block.shape[0]
            for k in range(block.shape[1] // part):
                start = pl.multiple_of((me_ref[0] ^ d ^ (base + k)) * part, part)
                rows_ref[d * cap : (d + 1) * cap, pl.ds(start, part)] = block[
                    :, k * part : (k + 1) * part
                ]
            base += block.shape[1] // part
    out_ref[...] = lax.dot_general(
        placing_ref[...], rows_ref[...], (((0,), (0,)), ((), ())), preferred_element_type=jnp.float32
    ).astype(jnp.bfloat16)


def ordered(me, d, chunks, part):
    rows = jnp.concatenate(chunks, axis=1)
    cap, width = rows.shape
    count = width // part
    order = me[0] ^ d ^ jnp.arange(count)
    return rows.reshape(cap, count, part)[:, order].reshape(cap, width)


def finished(me, placing, back, part):
    slots, tokens = placing.shape
    width = sum(block.shape[1] for block in back[0])
    if part % LANES:
        rows = [ordered(me, d, blocks, part) for d, blocks in enumerate(back)]
        return lax.dot_general(
            placing, jnp.concatenate(rows), (((0,), (0,)), ((), ())), preferred_element_type=jnp.float32
        ).astype(jnp.bfloat16)
    flat = [b for blocks in back for b in blocks]
    counts = [len(blocks) for blocks in back]
    return pl.pallas_call(
        functools.partial(finish_kernel, counts, part),
        out_shape=jax.ShapeDtypeStruct((tokens, width), jnp.bfloat16),
        in_specs=[pl.BlockSpec(memory_space=pltpu.SMEM)] + [VMEM] * (1 + len(flat)),
        out_specs=VMEM,
        scratch_shapes=[pltpu.VMEM((slots, width), jnp.bfloat16)],
        cost_estimate=cost(2 * slots * tokens * width, 2 * slots * width),
        name="finish",
    )(me, placing, *flat)


def sent(blocks, first):
    return [block if d == 0 else swap(block, "tp", d) for d, block in enumerate(blocks, start=first)]


def served(prompt, norm_gain, gate_master, up_master, down_master, group_pick, route_weight):
    groups, members = lax.axis_size("tp"), lax.axis_size("fs")
    width = prompt.shape[1]
    experts, _, part = gate_master.shape[1:]
    half = groups // 2
    me = lax.axis_index("tp").astype(jnp.int32).reshape(1)

    placing, send = route(me, prompt, group_pick, route_weight)
    rows = sent(send, 0)
    near, pairs, downs = rounded(me, norm_gain, gate_master, up_master, down_master, placing)
    near, pairs, downs = sent(near, 0), sent(pairs, half), sent(downs, half)

    near_rows, near_weights = stacked_rows(rows[:half], width)
    far_rows, far_weights = stacked_rows(rows[half:], width)
    weights = (near_weights, far_weights)
    firsts, seconds = gathered(near_rows, far_rows, "fs")
    all_rows = [r for pair in zip(firsts, seconds) for r in pair]
    cut = (groups - half) // 2
    sums = active_units(me, all_rows, near, 0, [], False)
    sums = active_units(me, all_rows, pairs[:cut], half, sums, False)
    active = active_units(me, all_rows, pairs[cut:], half + cut, sums, True)
    hiddens = [active[0]] + [swap(active[e], "fs", e) for e in range(1, members)]
    sides = gathered(*stacked_columns(near, 2), "fs")
    sets = [list(zip(*sides))]
    for blocks in (downs[:cut], downs[cut:]):
        whole = stacked_columns(blocks, 1)[0]
        sets.append([[one] for one in collected(whole, "fs")])
    early = mixed_rows(weights, hiddens, sets[:2], [], groups, experts)
    late = mixed_rows(weights, hiddens, sets[2:], early[:half], groups, experts)
    back = [[block] for block in sent(late[:half], 0)]
    back += zip(sent(early[half:], half), sent(late[half:], half))
    mixed = finished(me, placing, back, part)
    gate_serve, up_serve, down_serve = joined(me, near, pairs, downs)
    return (gate_serve, up_serve, down_serve, mixed)


def solution(mesh):
    placed = (
        P(("fs", "tp"), None),
        P("tp"),
        P(None, None, "fs", "tp"),
        P(None, None, "fs", "tp"),
        P(None, None, "fs", "tp"),
        P(("fs", "tp"), None),
        P(("fs", "tp"), None),
    )
    return jax.shard_map(
        served,
        mesh=mesh,
        in_specs=placed,
        out_specs=(
            P("tp", None, "fs", None),
            P("tp", None, "fs", None),
            P("tp", None, "fs", None),
            P(("fs", "tp"), None),
        ),
        check_vma=False,
    )
```

```python
import functools

import jax
import jax.numpy as jnp
from jax import lax
from jax.experimental import pallas as pl
from jax.experimental.pallas import tpu as pltpu
from jax.sharding import PartitionSpec as P


EPS = 1e-06
LANES = 128
BLOCKS = 2
ROOM = 16 << 20
VMEM = pl.BlockSpec(memory_space=pltpu.VMEM)


def nt_dot(left, right):
    return lax.dot_general(left, right, (((1,), (1,)), ((), ())), preferred_element_type=jnp.float32)


def cost(flops, moved):
    return pl.CostEstimate(flops=int(flops), bytes_accessed=int(moved), transcendentals=0)


def swap(value, axis, distance):
    count = lax.axis_size(axis)
    return lax.ppermute(value, axis, [(i, i ^ distance) for i in range(count)])


def route_kernel(cap, me_ref, prompt_ref, pick_ref, weight_ref, *out_refs):
    placing_ref, blocks = out_refs[0], out_refs[1:]
    slots, tokens = placing_ref.shape
    width = prompt_ref.shape[1]
    values = prompt_ref[...].astype(jnp.float32)
    scale = lax.rsqrt(jnp.mean(values * values, axis=1, keepdims=True) + EPS)
    normed = (values * scale).astype(jnp.bfloat16)
    distance = pick_ref[...] ^ me_ref[0]
    count = max(8, len(blocks))
    member = (lax.broadcasted_iota(jnp.int32, (count, tokens), 0) == distance).astype(jnp.float32)
    before = lax.broadcasted_iota(jnp.int32, (tokens, tokens), 0) < lax.broadcasted_iota(
        jnp.int32, (tokens, tokens), 1
    )
    earlier = jnp.dot(
        member.astype(jnp.bfloat16), before.astype(jnp.float32).astype(jnp.bfloat16),
        preferred_element_type=jnp.float32,
    )
    rank = jnp.sum(earlier * member, axis=0, keepdims=True).astype(jnp.int32)
    target = distance * cap + rank
    placing = (lax.broadcasted_iota(jnp.int32, (slots, tokens), 0) == target).astype(jnp.float32)
    placing = placing.astype(jnp.bfloat16)
    placing_ref[...] = placing
    weights = weight_ref[...].astype(jnp.float32)
    experts = weights.shape[0]
    row = lax.broadcasted_iota(jnp.int32, (LANES, tokens), 0)
    spread = jnp.zeros((LANES, tokens), jnp.float32)
    for x in range(experts):
        spread = jnp.where(row == x, weights[x : x + 1, :], spread)
    placed_weights = nt_dot(placing, spread.astype(jnp.bfloat16)).astype(jnp.bfloat16)
    rows = jnp.dot(placing, normed, preferred_element_type=jnp.float32).astype(jnp.bfloat16)
    for d, block in enumerate(blocks):
        block[:, :width] = rows[d * cap : (d + 1) * cap]
        block[:, width:] = placed_weights[d * cap : (d + 1) * cap]


def route(me, prompt, group_pick, route_weight):
    tokens, width = prompt.shape
    groups = lax.axis_size("tp")
    cap = 2 * tokens // groups
    block = jax.ShapeDtypeStruct((cap, width + LANES), jnp.bfloat16)
    outs = pl.pallas_call(
        functools.partial(route_kernel, cap),
        out_shape=[jax.ShapeDtypeStruct((groups * cap, tokens), jnp.bfloat16)] + [block] * groups,
        in_specs=[pl.BlockSpec(memory_space=pltpu.SMEM)] + [VMEM] * 3,
        out_specs=[VMEM] * (groups + 1),
        compiler_params=pltpu.CompilerParams(vmem_limit_bytes=ROOM),
        cost_estimate=cost(2 * groups * cap * tokens * width, 2 * tokens * width * 6),
        name="route",
    )(me, prompt, group_pick.reshape(1, tokens), route_weight.T)
    return outs[0], outs[1:]


def round_kernel(half, me_ref, gain_ref, gate_ref, up_ref, down_ref, *blocks):
    gain = gain_ref[...].reshape(1, 1, -1)
    near, far = blocks[:half], blocks[half:]
    for d in range(half + len(far) // 2):
        group = me_ref[0] ^ d
        pair, down = (near[d], near[d].at[2]) if d < half else (far[2 * (d - half)], far[2 * (d - half) + 1])
        pair[0] = (gate_ref[group] * gain).astype(jnp.bfloat16)
        pair[1] = (up_ref[group] * gain).astype(jnp.bfloat16)
        down[...] = down_ref[group].astype(jnp.bfloat16)


def rounded(me, gain, gate, up, down, after):
    groups, experts, units, part = gate.shape
    half = groups // 2
    shape = lambda *lead: jax.ShapeDtypeStruct((*lead, experts, units, part), jnp.bfloat16)
    size = 3 * groups * experts * units * part

    def kernel(me_ref, after_ref, *refs):
        round_kernel(half, me_ref, *refs)

    outs = pl.pallas_call(
        kernel,
        out_shape=[shape(3)] * half + [shape(2), shape()] * (groups - half),
        in_specs=[pl.BlockSpec(memory_space=pltpu.SMEM), pl.BlockSpec(memory_space=pl.ANY)] + [VMEM] * 4,
        out_specs=[VMEM] * (2 * groups - half),
        compiler_params=pltpu.CompilerParams(vmem_limit_bytes=ROOM),
        cost_estimate=cost(4 * size, 6 * size),
        name="rounding",
    )(me, after, gain.reshape(1, -1), gate, up, down)
    return outs[:half], outs[half::2], outs[half + 1 :: 2]


def parts_of(near, pairs, downs, which):
    if which == 2:
        return [ref[2] for ref in near] + list(downs)
    return [ref[which] for ref in near] + [ref[which] for ref in pairs]


def joined(me, near, pairs, downs):
    count = len(near) + len(pairs)
    _, experts, units, part = near[0].shape
    if part % LANES:
        order = me[0] ^ jnp.arange(count)
        outs = []
        for which in range(3):
            stack = jnp.stack(parts_of(near, pairs, downs, which))[order]
            outs.append(jnp.moveaxis(stack, 0, 2).reshape(1, experts, units, count * part))
        return outs
    sizes = (len(near), len(pairs), len(downs))

    def kernel(me_ref, *refs):
        ins, outs, sems = refs[: sum(sizes)], refs[sum(sizes) : -1], refs[-1]
        groups = ins[: sizes[0]], ins[sizes[0] : sizes[0] + sizes[1]], ins[sizes[0] + sizes[1] :]
        copies = []
        for which, out_ref in enumerate(outs):
            views = [[ref.at for ref in group] for group in groups[:2]]
            for d, piece in enumerate(parts_of(*views, groups[2], which)):
                start = pl.multiple_of((me_ref[0] ^ d) * part, part)
                copies.append(
                    pltpu.make_async_copy(
                        piece, out_ref.at[0, :, :, pl.ds(start, part)], sems.at[which, d]
                    )
                )
        for copy in copies:
            copy.start()
        for copy in copies:
            copy.wait()

    size = 3 * count * experts * units * part
    out = jax.ShapeDtypeStruct((1, experts, units, count * part), jnp.bfloat16)
    return pl.pallas_call(
        kernel,
        out_shape=[out] * 3,
        in_specs=[pl.BlockSpec(memory_space=pltpu.SMEM)] + [VMEM] * sum(sizes),
        out_specs=[pl.BlockSpec(memory_space=pl.ANY)] * 3,
        scratch_shapes=[pltpu.SemaphoreType.DMA((3, count))],
        compiler_params=pltpu.CompilerParams(vmem_limit_bytes=ROOM),
        cost_estimate=cost(4 * size, 4 * size),
        name="joining",
    )(me, *near, *pairs, *downs)


def stack_rows_kernel(width, *refs):
    blocks, rows_ref, weights_ref = refs[:-2], refs[-2], refs[-1]
    cap = blocks[0].shape[0]
    for d, block in enumerate(blocks):
        rows_ref[d * cap : (d + 1) * cap] = block[:, :width]
        weights_ref[d * cap : (d + 1) * cap] = block[:, width:]


def stacked_rows(blocks, width):
    count, cap = len(blocks), blocks[0].shape[0]
    return pl.pallas_call(
        functools.partial(stack_rows_kernel, width),
        out_shape=[
            jax.ShapeDtypeStruct((count * cap, width), jnp.bfloat16),
            jax.ShapeDtypeStruct((count * cap, LANES), jnp.bfloat16),
        ],
        in_specs=[VMEM] * count,
        out_specs=[VMEM] * 2,
        compiler_params=pltpu.CompilerParams(vmem_limit_bytes=ROOM),
        cost_estimate=cost(count * cap * width, 4 * count * cap * width),
        name="stack_rows",
    )(*blocks)


def stacked_columns(blocks, pieces):
    count = len(blocks)
    experts, units, part = blocks[0].shape[-3:]
    rows = experts * units // pieces
    moved = part % LANES == 0

    def kernel(*refs):
        ins, outs, sems = refs[:count], refs[count:-1], refs[-1]
        copies = []
        for d, block in enumerate(ins):
            piece = block.at[2] if len(block.shape) == 4 else block
            for x in range(experts):
                row = x * units % rows
                spot = (slice(row, row + units), slice(d * part, (d + 1) * part))
                out = outs[x * units // rows]
                if moved:
                    copies.append(pltpu.make_async_copy(piece.at[x], out.at[spot], sems.at[d, x]))
                else:
                    out[spot] = piece[x]
        for copy in copies:
            copy.start()
        for copy in copies:
            copy.wait()

    size = count * experts * units * part
    return pl.pallas_call(
        kernel,
        out_shape=[jax.ShapeDtypeStruct((rows, count * part), jnp.bfloat16)] * pieces,
        in_specs=[pl.BlockSpec(memory_space=pl.ANY) if moved else VMEM] * count,
        out_specs=[VMEM] * pieces,
        scratch_shapes=[pltpu.SemaphoreType.DMA((count, experts))],
        compiler_params=pltpu.CompilerParams(vmem_limit_bytes=ROOM),
        cost_estimate=cost(size, 4 * size),
        name="stack_columns",
    )(*blocks)


def collected(value, axis):
    count = lax.axis_size(axis)
    return [value] + [swap(value, axis, e) for e in range(1, count)]


def gathered(first, second, axis):
    count = lax.axis_size(axis)
    firsts, seconds = [first], [second]
    for e in range(1, count):
        low, high = e & -e, 1 << (e.bit_length() - 1)
        firsts.append(swap(firsts[e ^ low], axis, low))
        seconds.append(swap(seconds[e ^ high], axis, high))
    return firsts, seconds


def active_kernel(first, parts, counts, me_ref, *refs):
    pieces, refs = refs[: counts[0]], refs[counts[0] :]
    rows, before, refs = refs[: counts[1]], refs[counts[1] : counts[1] + counts[2]], refs[sum(counts[1:3]) :]
    outs, (matrix_ref, rows_ref, sums_ref, sems) = refs[: counts[3]], refs[counts[3] :]
    _, experts, units, part = pieces[0].shape
    both = experts * units
    width = rows_ref.shape[2]
    place = lax.shift_right_logical(me_ref[0] ^ first, parts.bit_length() - 1)
    columns = pl.ds(pl.multiple_of(place * width, width), width)
    slots = rows[0].shape[0]
    row_spot = lambda b: rows_ref.at[b * slots // rows_ref.shape[1], pl.ds(b * slots % rows_ref.shape[1], slots)]
    copies = [
        pltpu.make_async_copy(ref.at[:, columns], row_spot(b), sems.at[0, b]) for b, ref in enumerate(rows)
    ]
    copies += [
        pltpu.make_async_copy(ref, sums_ref.at[b], sems.at[1, b]) for b, ref in enumerate(before)
    ]
    fills = []
    for d, piece in enumerate(pieces):
        start = pl.multiple_of(((me_ref[0] & (len(pieces) - 1)) ^ d) * part, part)
        for which in range(2):
            for x in range(experts):
                row = which * both + x * units
                spot = matrix_ref.at[row : row + units, pl.ds(start, part)]
                sem = sems.at[2, (d * 2 + which) * experts + x]
                fills.append(pltpu.make_async_copy(piece.at[which, x], spot, sem))
    for copy in fills + copies:
        copy.start()
    for copy in fills:
        copy.wait()
    group = rows_ref.shape[1] // slots
    for m in range(rows_ref.shape[0]):
        mine = range(m * group, (m + 1) * group)
        for b in mine:
            copies[b].wait()
        pre = nt_dot(rows_ref[m], matrix_ref[...])
        for b in mine:
            place = (b - m * group) * slots
            part_pre = pre[place : place + slots]
            if before:
                copies[len(rows) + b].wait()
                part_pre = part_pre + sums_ref[b]
            if len(outs) == len(rows):
                outs[b][...] = part_pre
            else:
                gate, up = part_pre[:, :both], part_pre[:, both:]
                silu = gate / (1.0 + jnp.exp(-gate))
                place = b % 2 * slots
                outs[b // 2][place : place + slots, :] = (silu * up).astype(jnp.bfloat16)


def active_units(me, rows, pieces, first, before, last):
    _, experts, units, part = pieces[0].shape
    parts = len(pieces)
    if part % LANES:
        order = (me[0] % parts) ^ jnp.arange(parts)
        stack = jnp.stack([block[:2] for block in pieces])[order]
        pieces = [jnp.moveaxis(stack, 0, 3).reshape(2, experts, units, parts * part)]
    slots, width = rows[0].shape[0], parts * part
    count, both = len(rows), experts * units
    if last:
        outs = [jax.ShapeDtypeStruct((2 * slots, both), jnp.bfloat16)] * (count // 2)
    else:
        outs = [jax.ShapeDtypeStruct((slots, 2 * both), jnp.float32)] * count
    counts = (len(pieces), count, len(before), len(outs))
    return pl.pallas_call(
        functools.partial(active_kernel, first, parts, counts),
        out_shape=outs,
        in_specs=[pl.BlockSpec(memory_space=pltpu.SMEM)]
        + [pl.BlockSpec(memory_space=pl.ANY)] * (len(pieces) + count + len(before)),
        out_specs=[VMEM] * len(outs),
        scratch_shapes=[
            pltpu.VMEM((2 * both, width), jnp.bfloat16),
            pltpu.VMEM((BLOCKS, count * slots // BLOCKS, width), jnp.bfloat16),
            pltpu.VMEM((max(1, len(before)), slots, 2 * both), jnp.float32),
            pltpu.SemaphoreType.DMA((3, max(count, 2 * experts * len(pieces)))),
        ],
        compiler_params=pltpu.CompilerParams(vmem_limit_bytes=ROOM),
        cost_estimate=cost(4 * count * slots * both * width, 2 * count * slots * width),
        name="active",
    )(me, *pieces, *rows, *before)


def mix_kernel(members, experts, pieces, kept, near_ref, far_ref, *refs):
    hiddens, refs = refs[:members], refs[members:]
    number = members * sum(pieces)
    downs, kepts, outs = list(refs[:number]), refs[number : number + kept], refs[number + kept :]
    cap = outs[0].shape[0]
    for d, old in enumerate(kepts):
        outs[d][:, : old.shape[1]] = old[...]
    before = kepts[0].shape[1] if kept else 0
    begin = 0
    for piece in pieces:
        mine = [[downs.pop(0) for _ in range(piece)] for _ in range(members)]
        rows, width = mine[0][0].shape
        units = rows * piece // experts
        total = None
        for x in range(experts):
            row = x * units % rows
            hidden = jnp.concatenate([h[:, x * units : (x + 1) * units] for h in hiddens], axis=1)
            down = jnp.concatenate([d[x * units // rows][row : row + units] for d in mine], axis=0)
            term = jnp.dot(hidden, down, preferred_element_type=jnp.float32)
            weight = jnp.concatenate([near_ref[:, x : x + 1], far_ref[:, x : x + 1]], axis=0)
            term = term * weight.astype(jnp.float32)
            total = term if total is None else total + term
        total = total.astype(jnp.bfloat16)
        for d, out in enumerate(outs):
            place = begin + (before if d < kept else 0)
            out[:, place : place + width] = total[d * cap : (d + 1) * cap]
        begin += width


def mixed_rows(weights, hiddens, sets, kept, groups, experts):
    members = len(hiddens)
    slots = hiddens[0].shape[0]
    pieces = [len(downs[0]) for downs in sets]
    flat = [d for downs in sets for member in downs for d in member]
    width = sum(downs[0][0].shape[1] for downs in sets)
    cap = slots // groups
    before = kept[0].shape[1] if kept else 0
    out = lambda d: jax.ShapeDtypeStruct((cap, width + (before if d < len(kept) else 0)), jnp.bfloat16)
    size = members * hiddens[0].shape[1] * width
    return pl.pallas_call(
        functools.partial(mix_kernel, members, experts, pieces, len(kept)),
        out_shape=[out(d) for d in range(groups)],
        in_specs=[VMEM] * (2 + members + len(flat) + len(kept)),
        out_specs=[VMEM] * groups,
        compiler_params=pltpu.CompilerParams(vmem_limit_bytes=ROOM),
        cost_estimate=cost(2 * slots * size, 2 * size),
        name="mixing",
    )(*weights, *hiddens, *flat, *kept)


def finish_kernel(counts, part, me_ref, placing_ref, *refs):
    out_ref, rows_ref = refs[-2], refs[-1]
    blocks = list(refs[:-2])
    for d, count in enumerate(counts):
        base = 0
        for _ in range(count):
            block = blocks.pop(0)
            cap = block.shape[0]
            for k in range(block.shape[1] // part):
                start = pl.multiple_of((me_ref[0] ^ d ^ (base + k)) * part, part)
                rows_ref[d * cap : (d + 1) * cap, pl.ds(start, part)] = block[
                    :, k * part : (k + 1) * part
                ]
            base += block.shape[1] // part
    out_ref[...] = lax.dot_general(
        placing_ref[...], rows_ref[...], (((0,), (0,)), ((), ())), preferred_element_type=jnp.float32
    ).astype(jnp.bfloat16)


def ordered(me, d, chunks, part):
    rows = jnp.concatenate(chunks, axis=1)
    cap, width = rows.shape
    count = width // part
    order = me[0] ^ d ^ jnp.arange(count)
    return rows.reshape(cap, count, part)[:, order].reshape(cap, width)


def finished(me, placing, back, part):
    slots, tokens = placing.shape
    width = sum(block.shape[1] for block in back[0])
    if part % LANES:
        rows = [ordered(me, d, blocks, part) for d, blocks in enumerate(back)]
        return lax.dot_general(
            placing, jnp.concatenate(rows), (((0,), (0,)), ((), ())), preferred_element_type=jnp.float32
        ).astype(jnp.bfloat16)
    flat = [b for blocks in back for b in blocks]
    counts = [len(blocks) for blocks in back]
    return pl.pallas_call(
        functools.partial(finish_kernel, counts, part),
        out_shape=jax.ShapeDtypeStruct((tokens, width), jnp.bfloat16),
        in_specs=[pl.BlockSpec(memory_space=pltpu.SMEM)] + [VMEM] * (1 + len(flat)),
        out_specs=VMEM,
        scratch_shapes=[pltpu.VMEM((slots, width), jnp.bfloat16)],
        compiler_params=pltpu.CompilerParams(vmem_limit_bytes=ROOM),
        cost_estimate=cost(2 * slots * tokens * width, 2 * slots * width),
        name="finish",
    )(me, placing, *flat)


def sent(blocks, first):
    return [block if d == 0 else swap(block, "tp", d) for d, block in enumerate(blocks, start=first)]


def served(prompt, norm_gain, gate_master, up_master, down_master, group_pick, route_weight):
    groups, members = lax.axis_size("tp"), lax.axis_size("fs")
    width = prompt.shape[1]
    experts, _, part = gate_master.shape[1:]
    half = groups // 2
    me = lax.axis_index("tp").astype(jnp.int32).reshape(1)

    placing, send = route(me, prompt, group_pick, route_weight)
    rows = sent(send, 0)
    near, pairs, downs = rounded(me, norm_gain, gate_master, up_master, down_master, placing)
    near, pairs, downs = sent(near, 0), sent(pairs, half), sent(downs, half)

    near_rows, near_weights = stacked_rows(rows[:half], width)
    far_rows, far_weights = stacked_rows(rows[half:], width)
    weights = (near_weights, far_weights)
    firsts, seconds = gathered(near_rows, far_rows, "fs")
    all_rows = [r for pair in zip(firsts, seconds) for r in pair]
    cut = (groups - half) // 2
    sums = active_units(me, all_rows, near, 0, [], False)
    sums = active_units(me, all_rows, pairs[:cut], half, sums, False)
    active = active_units(me, all_rows, pairs[cut:], half + cut, sums, True)
    hiddens = [active[0]] + [swap(active[e], "fs", e) for e in range(1, members)]
    sides = gathered(*stacked_columns(near, 2), "fs")
    sets = [list(zip(*sides))]
    for blocks in (downs[:cut], downs[cut:]):
        whole = stacked_columns(blocks, 1)[0]
        sets.append([[one] for one in collected(whole, "fs")])
    early = mixed_rows(weights, hiddens, sets[:2], [], groups, experts)
    late = mixed_rows(weights, hiddens, sets[2:], early[:half], groups, experts)
    back = [[block] for block in sent(late[:half], 0)]
    back += zip(sent(early[half:], half), sent(late[half:], half))
    mixed = finished(me, placing, back, part)
    gate_serve, up_serve, down_serve = joined(me, near, pairs, downs)
    return (gate_serve, up_serve, down_serve, mixed)


def solution(mesh):
    placed = (
        P(("fs", "tp"), None),
        P("tp"),
        P(None, None, "fs", "tp"),
        P(None, None, "fs", "tp"),
        P(None, None, "fs", "tp"),
        P(("fs", "tp"), None),
        P(("fs", "tp"), None),
    )
    return jax.shard_map(
        served,
        mesh=mesh,
        in_specs=placed,
        out_specs=(
            P("tp", None, "fs", None),
            P("tp", None, "fs", None),
            P("tp", None, "fs", None),
            P(("fs", "tp"), None),
        ),
        check_vma=False,
    )
```

```python
import functools

import jax
import jax.numpy as jnp
from jax import lax
from jax.experimental import pallas as pl
from jax.experimental.pallas import tpu as pltpu
from jax.sharding import PartitionSpec as P


EPS = 1e-06
LANES = 128
BLOCKS = 1
ROOM = 16 << 20
VMEM = pl.BlockSpec(memory_space=pltpu.VMEM)
HBM = pl.BlockSpec(memory_space=pltpu.HBM)


def nt_dot(left, right):
    return lax.dot_general(left, right, (((1,), (1,)), ((), ())), preferred_element_type=jnp.float32)


def cost(flops, moved):
    return pl.CostEstimate(flops=int(flops), bytes_accessed=int(moved), transcendentals=0)


def swap(value, axis, distance):
    count = lax.axis_size(axis)
    return lax.ppermute(value, axis, [(i, i ^ distance) for i in range(count)])


def route_kernel(cap, me_ref, prompt_any, pick_any, weight_any, *refs):
    out_refs, (prompt_ref, pick_ref, weight_ref, sems) = refs[:-4], refs[-4:]
    copies = [
        pltpu.make_async_copy(source, spot, sems.at[n])
        for n, (source, spot) in enumerate(
            ((pick_any, pick_ref), (weight_any, weight_ref), (prompt_any, prompt_ref))
        )
    ]
    for copy in copies:
        copy.start()
    placing_ref = out_refs[0]
    count = (len(out_refs) - 1) // 2
    blocks, weight_blocks = out_refs[1 : 1 + count], out_refs[1 + count :]
    slots, tokens = placing_ref.shape
    for copy in copies:
        copy.wait()
    values = prompt_ref[...].astype(jnp.float32)
    scale = lax.rsqrt(jnp.mean(values * values, axis=1, keepdims=True) + EPS)
    normed = (values * scale).astype(jnp.bfloat16)
    distance = pick_ref[...] ^ me_ref[0]
    count = max(8, len(blocks))
    member = (lax.broadcasted_iota(jnp.int32, (count, tokens), 0) == distance).astype(jnp.float32)
    before = lax.broadcasted_iota(jnp.int32, (tokens, tokens), 0) < lax.broadcasted_iota(
        jnp.int32, (tokens, tokens), 1
    )
    earlier = jnp.dot(
        member.astype(jnp.bfloat16), before.astype(jnp.float32).astype(jnp.bfloat16),
        preferred_element_type=jnp.float32,
    )
    rank = jnp.sum(earlier * member, axis=0, keepdims=True).astype(jnp.int32)
    target = distance * cap + rank
    placing = (lax.broadcasted_iota(jnp.int32, (slots, tokens), 0) == target).astype(jnp.float32)
    placing = placing.astype(jnp.bfloat16)
    placing_ref[...] = placing
    weights = weight_ref[...].astype(jnp.float32)
    experts = weights.shape[0]
    row = lax.broadcasted_iota(jnp.int32, (LANES, tokens), 0)
    spread = jnp.zeros((LANES, tokens), jnp.float32)
    for x in range(experts):
        spread = jnp.where(row == x, weights[x : x + 1, :], spread)
    placed_weights = nt_dot(placing, spread.astype(jnp.bfloat16)).astype(jnp.bfloat16)
    rows = jnp.dot(placing, normed, preferred_element_type=jnp.float32).astype(jnp.bfloat16)
    for d, block in enumerate(blocks):
        block[...] = rows[d * cap : (d + 1) * cap]
        weight_blocks[d][...] = placed_weights[d * cap : (d + 1) * cap]


def route(me, prompt, group_pick, route_weight):
    tokens, width = prompt.shape
    groups = lax.axis_size("tp")
    cap = 2 * tokens // groups
    block = jax.ShapeDtypeStruct((cap, width), jnp.bfloat16)
    weight_block = jax.ShapeDtypeStruct((cap, LANES), jnp.bfloat16)
    experts = route_weight.shape[1]
    outs = pl.pallas_call(
        functools.partial(route_kernel, cap),
        out_shape=[jax.ShapeDtypeStruct((groups * cap, tokens), jnp.bfloat16)]
        + [block] * groups
        + [weight_block] * groups,
        in_specs=[pl.BlockSpec(memory_space=pltpu.SMEM)] + [HBM] * 3,
        out_specs=[VMEM] * (2 * groups + 1),
        scratch_shapes=[
            pltpu.VMEM((tokens, width), jnp.bfloat16),
            pltpu.VMEM((1, tokens), jnp.int32),
            pltpu.VMEM((experts, tokens), jnp.bfloat16),
            pltpu.SemaphoreType.DMA((3,)),
        ],
        compiler_params=pltpu.CompilerParams(vmem_limit_bytes=ROOM),
        cost_estimate=cost(2 * groups * cap * tokens * width, 2 * tokens * width * 6),
        name="route",
    )(me, prompt, group_pick.reshape(1, tokens), route_weight.T)
    return outs[0], outs[1 : 1 + groups], outs[1 + groups :]


def rounded(me, gain, gate, up, down, after):
    groups, experts, units, part = gate.shape
    half = groups // 2
    shape = lambda *lead: jax.ShapeDtypeStruct((*lead, experts, units, part), jnp.bfloat16)
    size = 3 * groups * experts * units * part

    def kernel(me_ref, after_ref, gain_ref, *refs):
        masters, blocks, values, sems = refs[:3], refs[3:-2], refs[-2], refs[-1]
        gains = gain_ref[...].reshape(1, 1, -1)
        near, far = blocks[:half], blocks[half:]
        copies = {}
        for d in range(groups):
            for which, master in enumerate(masters):
                copies[d, which] = pltpu.make_async_copy(
                    master.at[me_ref[0] ^ d], values.at[which, d], sems.at[which, d]
                )
                copies[d, which].start()
        for d in range(groups):
            pair, place = (near[d], near[d].at[2]) if d < half else far[2 * (d - half) :][:2]
            for which in range(2):
                copies[d, which].wait()
                pair[which] = (values[which, d] * gains).astype(jnp.bfloat16)
            copies[d, 2].wait()
            place[...] = values[2, d].astype(jnp.bfloat16)

    outs = pl.pallas_call(
        kernel,
        out_shape=[shape(3)] * half + [shape(2), shape()] * (groups - half),
        in_specs=[pl.BlockSpec(memory_space=pltpu.SMEM), pl.BlockSpec(memory_space=pl.ANY), VMEM]
        + [HBM] * 3,
        out_specs=[VMEM] * (2 * groups - half),
        scratch_shapes=[
            pltpu.VMEM((3, groups, experts, units, part), jnp.float32),
            pltpu.SemaphoreType.DMA((3, groups)),
        ],
        compiler_params=pltpu.CompilerParams(vmem_limit_bytes=ROOM),
        cost_estimate=cost(4 * size, 6 * size),
        name="rounding",
    )(me, after, gain.reshape(1, -1), gate, up, down)
    return outs[:half], outs[half::2], outs[half + 1 :: 2]


def parts_of(near, pairs, downs, which):
    if which == 2:
        return [ref[2] for ref in near] + list(downs)
    return [ref[which] for ref in near] + [ref[which] for ref in pairs]


def joined(me, near, pairs, downs):
    count = len(near) + len(pairs)
    _, experts, units, part = near[0].shape
    if part % LANES:
        order = me[0] ^ jnp.arange(count)
        outs = []
        for which in range(3):
            stack = jnp.stack(parts_of(near, pairs, downs, which))[order]
            outs.append(jnp.moveaxis(stack, 0, 2).reshape(1, experts, units, count * part))
        return outs
    sizes = (len(near), len(pairs), len(downs))

    def kernel(me_ref, *refs):
        ins, outs, sems = refs[: sum(sizes)], refs[sum(sizes) : -1], refs[-1]
        groups = ins[: sizes[0]], ins[sizes[0] : sizes[0] + sizes[1]], ins[sizes[0] + sizes[1] :]
        copies = []
        for which, out_ref in enumerate(outs):
            views = [[ref.at for ref in group] for group in groups[:2]]
            for d, piece in enumerate(parts_of(*views, groups[2], which)):
                start = pl.multiple_of((me_ref[0] ^ d) * part, part)
                copies.append(
                    pltpu.make_async_copy(
                        piece, out_ref.at[0, :, :, pl.ds(start, part)], sems.at[which, d]
                    )
                )
        for copy in copies:
            copy.start()
        for copy in copies:
            copy.wait()

    size = 3 * count * experts * units * part
    out = jax.ShapeDtypeStruct((1, experts, units, count * part), jnp.bfloat16)
    return pl.pallas_call(
        kernel,
        out_shape=[out] * 3,
        in_specs=[pl.BlockSpec(memory_space=pltpu.SMEM)] + [VMEM] * sum(sizes),
        out_specs=[pl.BlockSpec(memory_space=pl.ANY)] * 3,
        scratch_shapes=[pltpu.SemaphoreType.DMA((3, count))],
        compiler_params=pltpu.CompilerParams(vmem_limit_bytes=ROOM),
        cost_estimate=cost(4 * size, 4 * size),
        name="joining",
    )(me, *near, *pairs, *downs)


def stack_rows_kernel(*refs):
    blocks, rows_ref = refs[:-1], refs[-1]
    cap = blocks[0].shape[0]
    for d, block in enumerate(blocks):
        rows_ref[d * cap : (d + 1) * cap] = block[...]


def stacked_rows(blocks):
    count, (cap, width) = len(blocks), blocks[0].shape
    return pl.pallas_call(
        stack_rows_kernel,
        out_shape=jax.ShapeDtypeStruct((count * cap, width), jnp.bfloat16),
        in_specs=[VMEM] * count,
        out_specs=VMEM,
        compiler_params=pltpu.CompilerParams(vmem_limit_bytes=ROOM),
        cost_estimate=cost(count * cap * width, 4 * count * cap * width),
        name="stack_rows",
    )(*blocks)


def stacked_columns(blocks, pieces):
    count = len(blocks)
    experts, units, part = blocks[0].shape[-3:]
    rows = experts * units // pieces
    moved = part % LANES == 0

    def kernel(*refs):
        ins, outs, sems = refs[:count], refs[count:-1], refs[-1]
        copies = []
        for d, block in enumerate(ins):
            piece = block.at[2] if len(block.shape) == 4 else block
            for x in range(experts):
                row = x * units % rows
                spot = (slice(row, row + units), slice(d * part, (d + 1) * part))
                out = outs[x * units // rows]
                if moved:
                    copies.append(pltpu.make_async_copy(piece.at[x], out.at[spot], sems.at[d, x]))
                else:
                    out[spot] = piece[x]
        for copy in copies:
            copy.start()
        for copy in copies:
            copy.wait()

    size = count * experts * units * part
    return pl.pallas_call(
        kernel,
        out_shape=[jax.ShapeDtypeStruct((rows, count * part), jnp.bfloat16)] * pieces,
        in_specs=[pl.BlockSpec(memory_space=pl.ANY) if moved else VMEM] * count,
        out_specs=[VMEM] * pieces,
        scratch_shapes=[pltpu.SemaphoreType.DMA((count, experts))],
        compiler_params=pltpu.CompilerParams(vmem_limit_bytes=ROOM),
        cost_estimate=cost(size, 4 * size),
        name="stack_columns",
    )(*blocks)


def collected(value, axis):
    count = lax.axis_size(axis)
    return [value] + [swap(value, axis, e) for e in range(1, count)]


def gathered(first, second, axis):
    count = lax.axis_size(axis)
    firsts, seconds = [first], [second]
    for e in range(1, count):
        low, high = e & -e, 1 << (e.bit_length() - 1)
        firsts.append(swap(firsts[e ^ low], axis, low))
        seconds.append(swap(seconds[e ^ high], axis, high))
    return firsts, seconds


def active_kernel(first, parts, counts, me_ref, *refs):
    pieces, refs = refs[: counts[0]], refs[counts[0] :]
    rows, before, refs = refs[: counts[1]], refs[counts[1] : counts[1] + counts[2]], refs[sum(counts[1:3]) :]
    outs, (matrix_ref, rows_ref, sums_ref, sems) = refs[: counts[3]], refs[counts[3] :]
    _, experts, units, part = pieces[0].shape
    both = experts * units
    width = rows_ref.shape[2]
    place = lax.shift_right_logical(me_ref[0] ^ first, parts.bit_length() - 1)
    columns = pl.ds(pl.multiple_of(place * width, width), width)
    slots = rows[0].shape[0]
    row_spot = lambda b: rows_ref.at[b * slots // rows_ref.shape[1], pl.ds(b * slots % rows_ref.shape[1], slots)]
    copies = [
        pltpu.make_async_copy(ref.at[:, columns], row_spot(b), sems.at[0, b]) for b, ref in enumerate(rows)
    ]
    copies += [
        pltpu.make_async_copy(ref, sums_ref.at[b], sems.at[1, b]) for b, ref in enumerate(before)
    ]
    fills = []
    for d, piece in enumerate(pieces):
        start = pl.multiple_of(((me_ref[0] & (len(pieces) - 1)) ^ d) * part, part)
        for which in range(2):
            for x in range(experts):
                row = which * both + x * units
                spot = matrix_ref.at[row : row + units, pl.ds(start, part)]
                sem = sems.at[2, (d * 2 + which) * experts + x]
                fills.append(pltpu.make_async_copy(piece.at[which, x], spot, sem))
    for copy in fills + copies:
        copy.start()
    for copy in fills:
        copy.wait()
    group = rows_ref.shape[1] // slots
    for m in range(rows_ref.shape[0]):
        mine = range(m * group, (m + 1) * group)
        for b in mine:
            copies[b].wait()
        pre = nt_dot(rows_ref[m], matrix_ref[...])
        for b in mine:
            place = (b - m * group) * slots
            part_pre = pre[place : place + slots]
            if before:
                copies[len(rows) + b].wait()
                part_pre = part_pre + sums_ref[b]
            if len(outs) == len(rows):
                outs[b][...] = part_pre
            else:
                gate, up = part_pre[:, :both], part_pre[:, both:]
                silu = gate / (1.0 + jnp.exp(-gate))
                place = b % 2 * slots
                outs[b // 2][place : place + slots, :] = (silu * up).astype(jnp.bfloat16)


def active_units(me, rows, pieces, first, before, last):
    _, experts, units, part = pieces[0].shape
    parts = len(pieces)
    if part % LANES:
        order = (me[0] % parts) ^ jnp.arange(parts)
        stack = jnp.stack([block[:2] for block in pieces])[order]
        pieces = [jnp.moveaxis(stack, 0, 3).reshape(2, experts, units, parts * part)]
    slots, width = rows[0].shape[0], parts * part
    count, both = len(rows), experts * units
    if last:
        outs = [jax.ShapeDtypeStruct((2 * slots, both), jnp.bfloat16)] * (count // 2)
    else:
        outs = [jax.ShapeDtypeStruct((slots, 2 * both), jnp.float32)] * count
    counts = (len(pieces), count, len(before), len(outs))
    return pl.pallas_call(
        functools.partial(active_kernel, first, parts, counts),
        out_shape=outs,
        in_specs=[pl.BlockSpec(memory_space=pltpu.SMEM)]
        + [pl.BlockSpec(memory_space=pl.ANY)] * (len(pieces) + count + len(before)),
        out_specs=[VMEM] * len(outs),
        scratch_shapes=[
            pltpu.VMEM((2 * both, width), jnp.bfloat16),
            pltpu.VMEM((BLOCKS, count * slots // BLOCKS, width), jnp.bfloat16),
            pltpu.VMEM((max(1, len(before)), slots, 2 * both), jnp.float32),
            pltpu.SemaphoreType.DMA((3, max(count, 2 * experts * len(pieces)))),
        ],
        compiler_params=pltpu.CompilerParams(vmem_limit_bytes=ROOM),
        cost_estimate=cost(4 * count * slots * both * width, 2 * count * slots * width),
        name="active",
    )(me, *pieces, *rows, *before)


def mix_kernel(members, experts, pieces, kept, groups, *refs):
    weight_refs, refs = refs[:groups], refs[groups:]
    hiddens, refs = refs[:members], refs[members:]
    number = members * sum(pieces)
    downs, kepts, outs = list(refs[:number]), refs[number : number + kept], refs[number + kept :]
    cap = outs[0].shape[0]
    for d, old in enumerate(kepts):
        outs[d][:, : old.shape[1]] = old[...]
    before = kepts[0].shape[1] if kept else 0
    begin = 0
    for piece in pieces:
        mine = [[downs.pop(0) for _ in range(piece)] for _ in range(members)]
        rows, width = mine[0][0].shape
        units = rows * piece // experts
        total = None
        for x in range(experts):
            row = x * units % rows
            hidden = jnp.concatenate([h[:, x * units : (x + 1) * units] for h in hiddens], axis=1)
            down = jnp.concatenate([d[x * units // rows][row : row + units] for d in mine], axis=0)
            term = jnp.dot(hidden, down, preferred_element_type=jnp.float32)
            weight = jnp.concatenate([ref[:, x : x + 1].astype(jnp.float32) for ref in weight_refs], axis=0)
            term = term * weight
            total = term if total is None else total + term
        total = total.astype(jnp.bfloat16)
        for d, out in enumerate(outs):
            place = begin + (before if d < kept else 0)
            out[:, place : place + width] = total[d * cap : (d + 1) * cap]
        begin += width


def mixed_rows(weights, hiddens, sets, kept, groups, experts):
    members = len(hiddens)
    slots = hiddens[0].shape[0]
    pieces = [len(downs[0]) for downs in sets]
    flat = [d for downs in sets for member in downs for d in member]
    width = sum(downs[0][0].shape[1] for downs in sets)
    cap = slots // groups
    before = kept[0].shape[1] if kept else 0
    out = lambda d: jax.ShapeDtypeStruct((cap, width + (before if d < len(kept) else 0)), jnp.bfloat16)
    size = members * hiddens[0].shape[1] * width
    return pl.pallas_call(
        functools.partial(mix_kernel, members, experts, pieces, len(kept), groups),
        out_shape=[out(d) for d in range(groups)],
        in_specs=[VMEM] * (groups + members + len(flat) + len(kept)),
        out_specs=[VMEM] * groups,
        compiler_params=pltpu.CompilerParams(vmem_limit_bytes=ROOM),
        cost_estimate=cost(2 * slots * size, 2 * size),
        name="mixing",
    )(*weights, *hiddens, *flat, *kept)


def finish_kernel(counts, part, me_ref, placing_ref, *refs):
    out_ref, rows_ref = refs[-2], refs[-1]
    blocks = list(refs[:-2])
    for d, count in enumerate(counts):
        base = 0
        for _ in range(count):
            block = blocks.pop(0)
            cap = block.shape[0]
            for k in range(block.shape[1] // part):
                start = pl.multiple_of((me_ref[0] ^ d ^ (base + k)) * part, part)
                rows_ref[d * cap : (d + 1) * cap, pl.ds(start, part)] = block[
                    :, k * part : (k + 1) * part
                ]
            base += block.shape[1] // part
    out_ref[...] = lax.dot_general(
        placing_ref[...], rows_ref[...], (((0,), (0,)), ((), ())), preferred_element_type=jnp.float32
    ).astype(jnp.bfloat16)


def ordered(me, d, chunks, part):
    rows = jnp.concatenate(chunks, axis=1)
    cap, width = rows.shape
    count = width // part
    order = me[0] ^ d ^ jnp.arange(count)
    return rows.reshape(cap, count, part)[:, order].reshape(cap, width)


def finished(me, placing, back, part):
    slots, tokens = placing.shape
    width = sum(block.shape[1] for block in back[0])
    if part % LANES:
        rows = [ordered(me, d, blocks, part) for d, blocks in enumerate(back)]
        return lax.dot_general(
            placing, jnp.concatenate(rows), (((0,), (0,)), ((), ())), preferred_element_type=jnp.float32
        ).astype(jnp.bfloat16)
    flat = [b for blocks in back for b in blocks]
    counts = [len(blocks) for blocks in back]
    return pl.pallas_call(
        functools.partial(finish_kernel, counts, part),
        out_shape=jax.ShapeDtypeStruct((tokens, width), jnp.bfloat16),
        in_specs=[pl.BlockSpec(memory_space=pltpu.SMEM)] + [VMEM] * (1 + len(flat)),
        out_specs=VMEM,
        scratch_shapes=[pltpu.VMEM((slots, width), jnp.bfloat16)],
        compiler_params=pltpu.CompilerParams(vmem_limit_bytes=ROOM),
        cost_estimate=cost(2 * slots * tokens * width, 2 * slots * width),
        name="finish",
    )(me, placing, *flat)


def sent(blocks, first):
    return [block if d == 0 else swap(block, "tp", d) for d, block in enumerate(blocks, start=first)]


def served(prompt, norm_gain, gate_master, up_master, down_master, group_pick, route_weight):
    groups, members = lax.axis_size("tp"), lax.axis_size("fs")
    experts, _, part = gate_master.shape[1:]
    half = groups // 2
    me = lax.axis_index("tp").astype(jnp.int32).reshape(1)

    placing, send, weight_send = route(me, prompt, group_pick, route_weight)
    rows = sent(send, 0)
    row_weights = sent(weight_send, 0)
    near, pairs, downs = rounded(me, norm_gain, gate_master, up_master, down_master, placing)
    near, pairs, downs = sent(near, 0), sent(pairs, half), sent(downs, half)

    near_rows = stacked_rows(rows[:half])
    far_rows = stacked_rows(rows[half:])
    firsts, seconds = gathered(near_rows, far_rows, "fs")
    all_rows = [r for pair in zip(firsts, seconds) for r in pair]
    cut = (groups - half) // 2
    sums = active_units(me, all_rows, near, 0, [], False)
    sums = active_units(me, all_rows, pairs[:cut], half, sums, False)
    active = active_units(me, all_rows, pairs[cut:], half + cut, sums, True)
    hiddens = [active[0]] + [swap(active[e], "fs", e) for e in range(1, members)]
    sides = gathered(*stacked_columns(near, 2), "fs")
    sets = [list(zip(*sides))]
    for blocks in (downs[:cut], downs[cut:]):
        whole = stacked_columns(blocks, 1)[0]
        sets.append([[one] for one in collected(whole, "fs")])
    early = mixed_rows(row_weights, hiddens, sets[:2], [], groups, experts)
    late = mixed_rows(row_weights, hiddens, sets[2:], early[:half], groups, experts)
    back = [[block] for block in sent(late[:half], 0)]
    back += zip(sent(early[half:], half), sent(late[half:], half))
    mixed = finished(me, placing, back, part)
    gate_serve, up_serve, down_serve = joined(me, near, pairs, downs)
    return (gate_serve, up_serve, down_serve, mixed)


def solution(mesh):
    placed = (
        P(("fs", "tp"), None),
        P("tp"),
        P(None, None, "fs", "tp"),
        P(None, None, "fs", "tp"),
        P(None, None, "fs", "tp"),
        P(("fs", "tp"), None),
        P(("fs", "tp"), None),
    )
    return jax.shard_map(
        served,
        mesh=mesh,
        in_specs=placed,
        out_specs=(
            P("tp", None, "fs", None),
            P("tp", None, "fs", None),
            P("tp", None, "fs", None),
            P(("fs", "tp"), None),
        ),
        check_vma=False,
    )
```
